32 devices in a mesh: ep: 8 (over z, y), tp: 4 (over x, core).
Axes of the slice: x: 2, y: 2, z: 4, core: 2. Of those that a mesh axis runs over, the one named last changes fastest.
Arguments:
- mix_input: bfloat16 [8192, 2048], P(('ep', 'tp')), may hold values from -6 to 6
- mix_gain: float32 [2048], replicated, may hold values from 0.1 to 1.9
- pool_weight: bfloat16 [4, 512, 512], replicated, may hold values from -0.25 to 0.25
- pool_scale: float32 [2048], replicated, may hold values from 0.1 to 1.9
- moe_input: bfloat16 [4096, 2048], P(('ep', 'tp')), may hold values from -6 to 6
- moe_gain: float32 [2048], replicated, may hold values from 0.1 to 1.9
- expert_ids: int32 [4096, 4], P('ep'), may hold values from 0 to 15, all different within a row; in each aligned block of 128 rows (0 to 127, 128 to 255, ...) at most 48 rows name the same one
- route_score: float32 [4096, 4], P(('ep', 'tp')), may hold values from 0.05 to 1
- expert_gate: bfloat16 [16, 2048, 1024], P('ep', None, 'tp'), may hold values from -0.125 to 0.125
- expert_up: bfloat16 [16, 2048, 1024], P('ep', None, 'tp'), may hold values from -0.125 to 0.125
- expert_down: bfloat16 [16, 1024, 2048], P('ep', 'tp'), may hold values from -0.1875 to 0.1875
- shared_gate: bfloat16 [2048, 512], P(None, 'tp'), may hold values from -0.125 to 0.125
- shared_up: bfloat16 [2048, 512], P(None, 'tp'), may hold values from -0.125 to 0.125
- shared_down: bfloat16 [512, 2048], P('tp'), may hold values from -0.25 to 0.25
Outputs:
- mix_output: bfloat16 [8192, 2048], P(('ep', 'tp'))
- moe_output: bfloat16 [4096, 2048], P(('ep', 'tp'))
The draws below stay inside these ranges and needn't reach their ends.
Inputs may be any that keep to these rules, and one draw needn't show every extreme that they name: `expert_ids`: each row names 4 different experts. Within each aligned block of 128 rows (the tokens of one device) no expert is named by more than 48 rows, a bound that some block reaches.
All inputs are finite; a program needn't handle non-finite values.
Results may differ from the reference program's by a relative error of at most 0.012.
Values may be sent and summed in bfloat16 or wider, within the bound.
A program may use at most 192 MiB of HBM per device.

```python
import math
import jax
import jax.numpy as jnp
import numpy as np
from jax import lax

D = 2048
GROUP = 512
FF = 1024
SH = 512
EXPERTS = 16
TOPK = 4
TOK_B = 128
TOKENS_A = 8192
TOKENS_B = 4096
CAP = 48
N_TP = 4


def levels(own_key, dims, shards, least, high):
    factor_of = 1.0
    for dim, blocks in shards:
        draws = jax.random.uniform(jax.random.fold_in(jax.random.fold_in(own_key, 6), dim), (blocks,), jnp.float32, least / len(shards), high / len(shards))
        factor_of = factor_of * jnp.repeat(jnp.exp(draws), dims[dim] // blocks).reshape((-1,) + (1,) * (len(dims) - 1 - dim))
    return factor_of


def routed_block(own_key, own, number, rows, amount, top, most, slope):
    order = jax.random.permutation(own_key, amount)
    packed, ordinary = load_shares(amount, rows * top, most, slope, True), load_shares(amount, rows * top, most, slope, False)
    places = jnp.arange(amount)

    def named(sizes, rotation):
        used = int((sizes > 0).sum())
        fixed = max(1, used // 4)
        moved = fixed + (places - fixed + rotation * (used - fixed)) % max(1, amount - fixed)
        return jnp.zeros((amount,), jnp.int32).at[order[jnp.where(places < fixed, places, moved)]].set(jnp.asarray(sizes, jnp.int32))

    sizes = jnp.where(number % 4 == 0, named(packed, number // 4), named(ordinary, number - number // 4 - 1))
    mixed = jax.random.permutation(jax.random.fold_in(own, 3), amount)
    donor, sink = mixed[0:amount // 2 * 2:2], mixed[1:amount // 2 * 2:2]
    margin = jnp.minimum(sizes[donor] - 1, most - sizes[sink]) // 2
    margin = jnp.where((donor == order[0]) | (sink == order[0]) | (sizes[sink] == 0), 0, jnp.maximum(margin, 0))
    moved = jax.random.randint(jax.random.fold_in(own, 4), (amount // 2,), 0, 1 << 20) % (margin + 1)
    sizes = sizes.at[donor].add(-moved).at[sink].add(moved)
    members = jnp.searchsorted(jnp.cumsum(sizes), jnp.arange(rows * top), side="right").astype(jnp.int32)
    listing = members.reshape(top, rows).T
    listing = listing[jax.random.permutation(jax.random.fold_in(own, 1), rows)]
    rotation = jax.random.randint(jax.random.fold_in(own, 2), (rows, 1), 0, top)
    return jnp.take_along_axis(listing, (jnp.arange(top)[None, :] + rotation) % top, axis=1)


def load_shares(amount, total, most, skew, full):
    weights = [(1 << 20) // math.isqrt(standing ** skew) + 1 for standing in range(1, amount + 1)]
    largest = most if full else min(most, max(-(-total // amount), total * weights[0] // sum(weights)))
    least = 1 if total - largest >= amount - 1 else 0
    given, surplus = [largest] + [least] * (amount - 1), total - largest - least * (amount - 1)
    while surplus > 0:
        movable = [i for i in range(1, amount) if given[i] < largest] or [i for i in range(1, amount) if given[i] < most]
        whole, left = sum([weights[i] for i in movable]), surplus
        for i in movable:
            addition = min(most - given[i], max(1, left * weights[i] // whole), surplus)
            given[i] = given[i] + addition
            surplus = surplus - addition
    return np.array(given)


def scatter_about(rng, shape, scale, bound, pieces=(), held_as=jnp.bfloat16):
    entries = scale * jax.random.normal(rng, shape, jnp.float32)
    if pieces:
        entries = entries * levels(rng, shape, pieces, -0.22, 0.18)
    return jnp.clip(entries, -bound, bound).astype(held_as)


def setup_inputs(seed: int = 0) -> dict:
    splits = jax.random.split(jax.random.key(seed), 15)
    mix_input = scatter_about(splits[0], (TOKENS_A, D), 1.0, 6.0, ((0, 32),))
    mix_gain = jnp.clip(1.0 + 0.18 * jax.random.normal(splits[1], (D,), jnp.float32), 0.1, 1.9)
    pool_weight = scatter_about(splits[2], (4, GROUP, GROUP), GROUP ** -0.5, 0.25)
    pool_scale = jnp.clip(1.0 + 0.18 * jax.random.normal(splits[3], (D,), jnp.float32), 0.1, 1.9)
    moe_input = scatter_about(splits[4], (TOKENS_B, D), 1.0, 6.0, ((0, 32),))
    moe_gain = jnp.clip(1.0 + 0.18 * jax.random.normal(splits[5], (D,), jnp.float32), 0.1, 1.9)
    expert_ids_keys = jax.random.split(jax.random.fold_in(splits[6], 1), TOKENS_B // TOK_B)
    expert_ids_turns = jax.random.permutation(jax.random.fold_in(splits[6], 3), TOKENS_B // TOK_B)
    expert_ids = jax.vmap(lambda own, number: routed_block(jax.random.fold_in(splits[6], 2), own, number, TOK_B, EXPERTS, TOPK, CAP, 1))(expert_ids_keys, expert_ids_turns).reshape((TOKENS_B, TOPK))
    route_score = jnp.clip(jnp.exp(math.log(1.0) - 2.9957323 * jax.random.uniform(splits[7], (TOKENS_B, TOPK), jnp.float32) ** levels(splits[7], (TOKENS_B, TOPK), ((0, 32),), -0.2, 0.2)), 0.05, 1.0)
    expert_gate = scatter_about(splits[8], (EXPERTS, D, FF), D ** -0.5, 0.125, ((0, 8), (2, 4)))
    expert_up = scatter_about(splits[9], (EXPERTS, D, FF), D ** -0.5, 0.125, ((0, 8), (2, 4)))
    expert_down = scatter_about(splits[10], (EXPERTS, FF, D), FF ** -0.5, 0.1875, ((0, 8), (1, 4)))
    shared_gate = scatter_about(splits[11], (D, SH), D ** -0.5, 0.125, ((1, 4),))
    shared_up = scatter_about(splits[12], (D, SH), D ** -0.5, 0.125, ((1, 4),))
    shared_down = scatter_about(splits[13], (SH, D), SH ** -0.5, 0.25, ((0, 4),))
    return dict(mix_input=mix_input, mix_gain=mix_gain, pool_weight=pool_weight, pool_scale=pool_scale, moe_input=moe_input, moe_gain=moe_gain, expert_ids=expert_ids, route_score=route_score, expert_gate=expert_gate, expert_up=expert_up, expert_down=expert_down, shared_gate=shared_gate, shared_up=shared_up, shared_down=shared_down)


WINDOWS = (2, 4, 8, 16)
RMS_EPS = 1e-06
ROUTED_SCALE = 2.5

def rms_norm(values, gain_row):
    upcast = values.astype(jnp.float32)
    scaled = upcast * lax.rsqrt(lax.optimization_barrier(jnp.mean(upcast * upcast, axis=-1, keepdims=True)) + RMS_EPS)
    return (scaled * gain_row).astype(jnp.bfloat16)

def rounded(values):
    return lax.optimization_barrier(values.astype(jnp.bfloat16)).astype(jnp.float32)

def window_means(normed, before, offset):
    row_count = normed.shape[0]
    lead_rows = before.shape[0]
    group_size = normed.shape[1] // len(WINDOWS)
    joined = jnp.concatenate([before, normed], axis=0).astype(jnp.float32)
    positions = offset + jnp.arange(row_count, dtype=jnp.int32)
    window_avg = []
    for group_idx, span in enumerate(WINDOWS):
        channels = joined[:, group_idx * group_size:(group_idx + 1) * group_size]
        first_row = lead_rows - span + 1
        running = channels[first_row:first_row + row_count]
        for shift_idx in range(1, span):
            running = running + channels[first_row + shift_idx:first_row + shift_idx + row_count]
        counts = jnp.minimum(positions + 1, span).astype(jnp.float32)
        window_avg.append(running / counts[:, None])
    return jnp.stack(window_avg, axis=1)

def width_sum(hidden, down_rows, block_width):
    summed = jnp.zeros((hidden.shape[0], down_rows.shape[1]), jnp.float32)
    for part_idx in range(N_TP):
        piece_out = jnp.dot(hidden[:, part_idx * block_width:(part_idx + 1) * block_width], down_rows[part_idx * block_width:(part_idx + 1) * block_width], preferred_element_type=jnp.float32)
        summed = summed + rounded(piece_out)
    return summed.astype(jnp.bfloat16)

def reference(mix_input, mix_gain, pool_weight, pool_scale, moe_input, moe_gain, expert_ids, route_score, expert_gate, expert_up, expert_down, shared_gate, shared_up, shared_down):
    normed = rms_norm(mix_input, mix_gain)
    row_count, width_all = normed.shape
    reach_rows = max(WINDOWS) - 1
    before = jnp.zeros((reach_rows, width_all), jnp.bfloat16)
    pooled = window_means(normed, before, 0)
    difference = (pooled - normed.astype(jnp.float32).reshape(row_count, len(WINDOWS), -1)).astype(jnp.bfloat16)
    mixed_out = jnp.einsum('sgc,gcd->sgd', difference.astype(jnp.float32), pool_weight.astype(jnp.float32))
    mix_output = (mixed_out.reshape(row_count, width_all) * pool_scale).astype(jnp.bfloat16)
    tok_count = moe_input.shape[0]
    h_moe = rms_norm(moe_input, moe_gain)
    block_count = tok_count // TOK_B
    pair_ids = expert_ids.reshape(block_count, TOK_B * TOPK)
    onehot = (pair_ids[:, :, None] == jnp.arange(EXPERTS, dtype=jnp.int32)[None, None, :]).astype(jnp.int32)
    rank = lax.optimization_barrier(jnp.sum((jnp.cumsum(onehot, axis=1) - onehot) * onehot, axis=2))
    block_idx = jnp.arange(block_count, dtype=jnp.int32)[:, None]
    slot_col = block_idx * CAP + rank
    owner = block_idx * TOK_B + jnp.arange(TOK_B * TOPK, dtype=jnp.int32)[None, :] // TOPK
    table = jnp.full((EXPERTS, block_count * CAP), tok_count, jnp.int32).at[pair_ids, slot_col].set(owner)
    padded = jnp.concatenate([h_moe, jnp.zeros((1, D), jnp.bfloat16)], axis=0)

    def run_expert(index):
        picked = padded[table[index]]
        gate_val = jnp.dot(picked, expert_gate[index], preferred_element_type=jnp.float32)
        up_val = jnp.dot(picked, expert_up[index], preferred_element_type=jnp.float32)
        hidden = (jax.nn.silu(gate_val) * up_val).astype(jnp.bfloat16)
        return width_sum(hidden, expert_down[index], FF // N_TP)
    results = lax.map(run_expert, jnp.arange(EXPERTS, dtype=jnp.int32))
    flat_res = results.reshape(EXPERTS * block_count * CAP, D)
    flat_idx = (pair_ids * (block_count * CAP) + slot_col).reshape(tok_count, TOPK)
    shared_gate_val = jnp.dot(h_moe, shared_gate, preferred_element_type=jnp.float32)
    shared_up_val = jnp.dot(h_moe, shared_up, preferred_element_type=jnp.float32)
    shared_hidden = (jax.nn.silu(shared_gate_val) * shared_up_val).astype(jnp.bfloat16)
    shared_out = width_sum(shared_hidden, shared_down, SH // N_TP)
    route_w = route_score / lax.optimization_barrier(jnp.sum(route_score, axis=1, keepdims=True)) * ROUTED_SCALE
    combined = shared_out.astype(jnp.float32)
    for pick_idx in range(TOPK):
        combined = combined + route_w[:, pick_idx:pick_idx + 1] * flat_res[flat_idx[:, pick_idx]].astype(jnp.float32)
    return (mix_output, combined.astype(jnp.bfloat16))
```

```python
import functools

import jax
import jax.numpy as jnp
from jax import lax
from jax.experimental import pallas as pl
from jax.experimental.pallas import tpu as pltpu
from jax.sharding import PartitionSpec as P

WINDOWS = (2, 4, 8, 16)
RMS_EPS = 1e-06
ROUTED_SCALE = 2.5


def passed_along(value, axis, by):
    length = lax.axis_size(axis)
    pairs = [(i, i + by) for i in range(length) if 0 <= i + by < length]
    return lax.ppermute(value, axis, pairs)


def rms_norm(values, gain_row):
    upcast = values.astype(jnp.float32)
    scaled = upcast * lax.rsqrt(jnp.mean(upcast * upcast, axis=-1, keepdims=True) + RMS_EPS)
    return (scaled * gain_row).astype(jnp.bfloat16)


def rounded(values):
    return lax.optimization_barrier(values.astype(jnp.bfloat16)).astype(jnp.float32)


def window_means(normed, before, offset):
    row_count = normed.shape[0]
    lead_rows = before.shape[0]
    group_size = normed.shape[1] // len(WINDOWS)
    joined = jnp.concatenate([before, normed], axis=0).astype(jnp.float32)
    positions = offset + jnp.arange(row_count, dtype=jnp.int32)
    window_avg = []
    for group_idx, span in enumerate(WINDOWS):
        channels = joined[:, group_idx * group_size : (group_idx + 1) * group_size]
        first_row = lead_rows - span + 1
        running = channels[first_row : first_row + row_count]
        for shift_idx in range(1, span):
            running = running + channels[first_row + shift_idx : first_row + shift_idx + row_count]
        counts = jnp.minimum(positions + 1, span).astype(jnp.float32)
        window_avg.append(running / counts[:, None])
    return jnp.stack(window_avg, axis=1)


def fill_slots(normed, picks, expert_count, capacity):
    tok_count, top_count = picks.shape
    pair_count = tok_count * top_count
    flat_ids = picks.reshape(pair_count)
    matches = flat_ids[:, None] == jnp.arange(expert_count, dtype=jnp.int32)[None, :]
    pair_line = jnp.arange(pair_count, dtype=jnp.int32)
    lower_mask = (pair_line[:, None] > pair_line[None, :]).astype(jnp.bfloat16)
    seen_before = jnp.dot(
        lower_mask, matches.astype(jnp.bfloat16), preferred_element_type=jnp.float32
    )
    rank = jnp.sum(seen_before * matches.astype(jnp.float32), axis=1).astype(jnp.int32)
    slots = flat_ids * capacity + rank
    owner = pair_line // top_count
    slot_token = jnp.full((expert_count * capacity,), tok_count, jnp.int32).at[slots].set(owner)
    padded = jnp.concatenate([normed, jnp.zeros((1, normed.shape[1]), normed.dtype)], axis=0)
    return (padded[slot_token], slots.reshape(tok_count, top_count))


def blockwise_down(hidden, down_rows, pieces, contract):
    block_width = hidden.shape[-1] // pieces
    summed = None
    for part_idx in range(pieces):
        piece_out = jnp.einsum(
            contract,
            hidden[..., part_idx * block_width : (part_idx + 1) * block_width],
            down_rows[..., part_idx * block_width : (part_idx + 1) * block_width, :],
            preferred_element_type=jnp.float32,
        )
        summed = rounded(piece_out) if summed is None else summed + rounded(piece_out)
    return summed.astype(jnp.bfloat16)


def routed_by_slots(h_moe, expert_ids, route_w, expert_gate, expert_up, expert_down, shared_gate, shared_up, shared_down):
    tok_count, model_width = h_moe.shape
    top_count = expert_ids.shape[1]
    quarters = lax.axis_size("tp")
    my_quarter = lax.axis_index("tp")
    ep_count = lax.axis_size("ep")
    local_experts = expert_gate.shape[0]
    expert_count = ep_count * local_experts
    capacity = 3 * tok_count * top_count // (2 * expert_count)
    per_source = local_experts * capacity
    full_gate, full_up, full_down, full_sgate, full_sup, full_sdown = (
        lax.all_gather(expert_gate, "tp", axis=2, tiled=True),
        lax.all_gather(expert_up, "tp", axis=2, tiled=True),
        lax.all_gather(expert_down, "tp", axis=1, tiled=True),
        lax.all_gather(shared_gate, "tp", axis=1, tiled=True),
        lax.all_gather(shared_up, "tp", axis=1, tiled=True),
        lax.all_gather(shared_down, "tp", axis=0, tiled=True),
    )
    my_ids = lax.dynamic_slice_in_dim(expert_ids, my_quarter * tok_count, tok_count, 0)
    outgoing, my_slots = fill_slots(h_moe, my_ids, expert_count, capacity)
    landed = lax.all_to_all(
        outgoing.reshape(ep_count, per_source, model_width),
        "ep",
        split_axis=0,
        concat_axis=0,
        tiled=True,
    )
    routed_in = landed.reshape(ep_count, local_experts, capacity, model_width)
    gate_val = jnp.einsum(
        "necd,edf->necf", routed_in, full_gate, preferred_element_type=jnp.float32
    )
    up_val = jnp.einsum("necd,edf->necf", routed_in, full_up, preferred_element_type=jnp.float32)
    hidden = (jax.nn.silu(gate_val) * up_val).astype(jnp.bfloat16)
    expert_back = blockwise_down(hidden, full_down, quarters, "necf,efd->necd")
    expert_back = expert_back.reshape(ep_count, per_source, model_width)
    shared_gate_val = jnp.dot(h_moe, full_sgate, preferred_element_type=jnp.float32)
    shared_up_val = jnp.dot(h_moe, full_sup, preferred_element_type=jnp.float32)
    shared_hidden = (jax.nn.silu(shared_gate_val) * shared_up_val).astype(jnp.bfloat16)
    shared_back = blockwise_down(shared_hidden, full_sdown, quarters, "tf,fd->td")
    returned = lax.all_to_all(expert_back, "ep", split_axis=0, concat_axis=0, tiled=True)
    returned = returned.reshape(expert_count * capacity, model_width)
    combined = shared_back.astype(jnp.float32)
    for pick_idx in range(top_count):
        combined = combined + route_w[:, pick_idx : pick_idx + 1] * returned[
            my_slots[:, pick_idx]
        ].astype(jnp.float32)
    return combined.astype(jnp.bfloat16)


COORD = {"z": 0, "y": 1, "x": 2}
HALO = 16


def all_blocks(z_count):
    return [(dz, dy, dx) for dz in range(z_count) for dy in range(2) for dx in range(2)]


def flat(block):
    return block[0] * 4 + block[1] * 2 + block[2]


def gather_edge(order, block):
    for dim in reversed(order):
        if block[COORD[dim]]:
            came = list(block)
            came[COORD[dim]] -= 1
            return dim, tuple(came)


def reduce_edge(order, block, z_count):
    for dim in reversed(order):
        if block[COORD[dim]]:
            goes = list(block)
            goes[COORD[dim]] = (block[0] + 1) % z_count if dim == "z" else 0
            return dim, tuple(goes)


def plan_steps(parts, z_count, units, block_us):
    blocks = all_blocks(z_count)
    home = blocks[0]
    groups = [[b for b in blocks if b[0] == dz] for dz in range(z_count)]
    gather, reduce_to = {}, {}
    below, feeds = {}, {}
    for part, (_, width, order) in enumerate(parts):
        for b in blocks[1:]:
            gather[part, b] = gather_edge(order, b)
            below.setdefault((part, gather[part, b][1]), []).append(b)
            reduce_to[part, b] = reduce_edge(order, b, z_count)
            feeds.setdefault((part, reduce_to[part, b][1]), []).append(b)

    def weight(part, b):
        return 1 + sum(weight(part, q) for q in below.get((part, b), []))

    clock, steps, flying = 3.0, [], []
    link = {"x": 0.0, "y": 0.0, "z": 0.0}
    have = {(part, home) for part in range(len(parts))}
    added, sent, computed = {}, set(), set()
    share = [part[1] / sum(p[1] for p in parts) for part in parts]

    def launch(kind, part, b, dim):
        steps.append((kind + "_send", part, b))
        begin = max(clock, link[dim])
        link[dim] = begin + share[part] * block_us
        flying.append((link[dim] + 2.3, kind, part, b))

    def forward(part, b):
        for q in sorted(below.get((part, b), []), key=lambda q: -weight(part, q)):
            launch("gather", part, q, gather[part, q][0])

    def pass_on(part, b):
        whole = added.get((part, b), 0) == len(feeds.get((part, b), []))
        if b != home and b in computed and whole and (part, b) not in sent:
            sent.add((part, b))
            launch("reduce", part, b, reduce_to[part, b][0])

    for part in range(len(parts)):
        forward(part, home)
    turn, unit, mixes = 0, 0, 1 + len(WINDOWS)
    mixed = 0
    while sum(added.values()) < len(parts) * (len(blocks) - 1):
        ready = sorted(m for m in flying if m[0] <= clock)
        ready = [m for m in ready if m[1] == "gather"] + [
            m for m in ready if m[1] == "reduce" and reduce_to[m[2], m[3]][1] in computed
        ]
        if ready:
            flying.remove(ready[0])
            _, kind, part, b = ready[0]
            if kind == "gather":
                steps.append(("gather_wait", part, b))
                have.add((part, b))
                forward(part, b)
            else:
                goes = reduce_to[part, b][1]
                steps.append(("reduce_add", part, b))
                clock += share[part]
                added[part, goes] = added.get((part, goes), 0) + 1
                pass_on(part, goes)
        elif turn < z_count and all(
            (part, b) in have for part in range(len(parts)) for b in groups[turn]
        ):
            steps.append(("unit", turn, unit))
            clock += units[unit]
            unit += 1
            if unit == len(units):
                computed.update(groups[turn])
                for part in range(len(parts)):
                    for b in groups[turn]:
                        pass_on(part, b)
                turn, unit = turn + 1, 0
        else:
            arrival = min(m[0] for m in flying if m[0] > clock)
            if mixed < mixes and arrival - clock > 0.3:
                steps.append(("mix", mixed, None))
                mixed += 1
                clock += 1.2
            else:
                clock = arrival
    steps.extend(("mix", i, None) for i in range(mixed, mixes))
    return steps, reduce_to, feeds, gather


def norm_rows(source, gain_ref, target, row_count, target_row):
    rows = 32

    def one(i, _):
        start = pl.multiple_of(i * rows, rows)
        upcast = source[pl.ds(start, rows), :].astype(jnp.float32)
        scaled = upcast * lax.rsqrt(jnp.mean(upcast * upcast, axis=-1, keepdims=True) + RMS_EPS)
        goes = pl.multiple_of(start + target_row, 16)
        target[pl.ds(goes, rows), :] = (scaled * gain_ref[...]).astype(jnp.bfloat16)
        return 0

    lax.fori_loop(0, row_count // rows, one, 0)


def kernel(
    sizes,
    mix_in,
    mix_gain,
    pool_w,
    pool_scale,
    moe_in,
    moe_gain,
    ids_ref,
    score_ref,
    gate_in,
    up_in,
    down_in,
    sgate_in,
    sup_in,
    sdown_in,
    mix_out,
    moe_out,
    rows_buf,
    sums_buf,
    land_buf,
    share_own,
    share_all,
    share_cols,
    gate_buf,
    up_buf,
    down_buf,
    sgate_buf,
    sup_buf,
    sdown_buf,
    hidden_buf,
    shared_hidden,
    moe_buf,
    mix_buf,
    pool_buf,
    normed_buf,
    diff_buf,
    local_sem,
    swap_send,
    swap_recv,
    share_send,
    share_recv,
    gather_send,
    gather_recv,
    reduce_send,
    reduce_recv,
    halo_send,
    halo_recv,
):
    z_count, tok, width, local, wide, swide, top = sizes
    ep_count, tp_count = 2 * z_count, 4
    my_ep, my_tp = lax.axis_index("ep"), lax.axis_index("tp")
    my_z, my_y, my_x, my_core = my_ep // 2, my_ep % 2, my_tp // 2, my_tp % 2
    partner = (my_ep, my_x * 2 + (1 - my_core))
    device_count = ep_count * tp_count
    my_flat = my_ep * tp_count + my_tp
    blocks = all_blocks(z_count)

    def spot(block):
        z = (my_z + block[0]) % z_count
        y = (my_y + block[1]) % 2
        x = (my_x + block[2]) % 2
        return (z * 2 + y, x * 2 + my_core)

    def at_flat(index):
        index = (index + device_count) % device_count
        return (index // tp_count, index % tp_count)

    loads = []

    def load(source, target):
        copy = pltpu.make_async_copy(source, target, local_sem.at[len(loads)])
        copy.start()
        loads.append(copy)
        return copy

    moe_load = load(moe_in, moe_buf)
    mix_load = load(mix_in, mix_buf)
    swaps = []
    half = width // 2
    pairs = []
    for e in range(local):
        for source, target in ((gate_in, gate_buf), (up_in, up_buf)):
            pairs.append((source.at[e], target.at[e, 0], target.at[e, 1]))
    pairs.append((sgate_in, sgate_buf.at[:, pl.ds(0, swide)], sgate_buf.at[:, pl.ds(swide, swide)]))
    pairs.append((sup_in, sup_buf.at[:, pl.ds(0, swide)], sup_buf.at[:, pl.ds(swide, swide)]))
    pairs.append((sdown_in, sdown_buf.at[pl.ds(0, swide)], sdown_buf.at[pl.ds(swide, swide)]))
    for e in range(local):
        pairs.append((down_in.at[e], down_buf.at[e, 0], down_buf.at[e, 1]))
    weight_loads = [load(source, own) for source, own, _ in pairs]
    pool_load = load(pool_w, pool_buf)

    barrier = pltpu.get_barrier_semaphore()
    outer = at_flat(my_flat + 2 * my_core - 1)
    peers = [spot(b) for b in blocks[1:]] + [partner, outer]
    for peer in peers:
        pl.semaphore_signal(barrier, inc=1, device_id=peer, device_id_type=pl.DeviceIdType.MESH)

    moe_load.wait()
    norm_rows(moe_buf, moe_gain, rows_buf.at[0], tok, 0)

    ids = ids_ref[pl.ds(pl.multiple_of(my_tp * tok, tok), tok), :]
    scores = score_ref[...]
    route_w = scores / jnp.sum(scores, axis=1, keepdims=True) * ROUTED_SCALE
    lane = lax.broadcasted_iota(jnp.int32, (tok, 128), 1)
    named = jnp.where(lane % 8 < local, (lane // 8) * local + lane % 8, -1)
    share = jnp.zeros((tok, 128), jnp.float32)
    for pick in range(top):
        share = share + jnp.where(
            ids[:, pick : pick + 1] == named, route_w[:, pick : pick + 1], 0.0
        )
    share_own[...] = share.T

    pl.semaphore_wait(barrier, len(peers))

    def remote(source, target, send, recv, device):
        copy = pltpu.make_async_remote_copy(
            src_ref=source,
            dst_ref=target,
            send_sem=send,
            recv_sem=recv,
            device_id=device,
            device_id_type=pl.DeviceIdType.MESH,
        )
        return copy

    started = []

    def go(copy):
        copy.start()
        started.append(copy)
        return copy

    shares = {}
    for b in blocks[1:]:
        z, y = (my_z + b[0]) % z_count, (my_y + b[1]) % 2
        row = pl.multiple_of((z * 2 + y) * 8, 8)
        shares[b] = go(
            remote(
                share_own.at[pl.ds(row, 8)],
                share_all.at[pl.ds(flat(b) * 8, 8)],
                share_send.at[flat(b)],
                share_recv.at[flat(b)],
                spot(b),
            )
        )
    for i, (source, _, other) in enumerate(pairs):
        swaps.append(go(remote(source, other, swap_send.at[i], swap_recv.at[i], partner)))

    parts = sizes_parts(width)
    steps, reduce_to, feeds, gather = plan_steps(
        parts, z_count, unit_times(local), tok * width * 2 / 46.6e3
    )
    toward = {"z": (1, 0, 0), "y": (0, 1, 0), "x": (0, 0, 1)}

    def gather_copy(part, b):
        start, count, _ = parts[part]
        dim, came = gather[part, b]
        cols = pl.ds(start, count)
        slot = part * len(blocks) + flat(b)
        return remote(
            rows_buf.at[flat(came), :, cols],
            rows_buf.at[flat(b), :, cols],
            gather_send.at[slot],
            gather_recv.at[slot],
            spot(toward[dim]),
        )

    def reduce_copy(part, b):
        start, count, _ = parts[part]
        dim, _ = reduce_to[part, b]
        cols = pl.ds(start, count)
        slot = part * len(blocks) + flat(b)
        return remote(
            sums_buf.at[flat(b), :, cols],
            land_buf.at[flat(b), :, cols],
            reduce_send.at[slot],
            reduce_recv.at[slot],
            spot(toward[dim]),
        )

    rows_per = 4 * tok
    span = 2 * wide

    def first_unit():
        own_row = pl.multiple_of(my_ep * 8, 8)
        share_all[pl.ds(0, 8), :] = share_own[pl.ds(own_row, 8), :]
        for b in blocks[1:]:
            shares[b].wait_recv()
        share_cols[...] = share_all[...].T

    def hidden_unit(turn, unit):
        e, side = unit // 2, unit % 2
        if turn == 0:
            if unit == 0:
                first_unit()
            for i in (2 * e, 2 * e + 1):
                if side == 0:
                    weight_loads[i].wait()
                else:
                    swaps[i].wait_recv()
        gate_w, up_w = gate_buf.at[e, side], up_buf.at[e, side]
        for piece in range(2):
            rows = rows_buf[turn * 4 + 2 * piece : turn * 4 + 2 * piece + 2].reshape(2 * tok, width)
            gate_val = jnp.dot(rows, gate_w[...], preferred_element_type=jnp.float32)
            up_val = jnp.dot(rows, up_w[...], preferred_element_type=jnp.float32)
            column = [
                share_cols[:, (turn * 4 + 2 * piece + i) * 8 + e : (turn * 4 + 2 * piece + i) * 8 + e + 1]
                for i in range(2)
            ]
            column = jnp.concatenate(column, axis=0)
            hidden = (jax.nn.silu(gate_val) * up_val * column).astype(jnp.bfloat16)
            hidden_buf[
                piece * 2 * tok : (piece + 1) * 2 * tok, unit * wide : (unit + 1) * wide
            ] = hidden

    def shared_unit():
        for i in range(2 * local, 2 * local + 2):
            weight_loads[i].wait()
            swaps[i].wait_recv()
        rows = rows_buf[0:2].reshape(2 * tok, width)
        gate_val = jnp.dot(rows, sgate_buf[...], preferred_element_type=jnp.float32)
        up_val = jnp.dot(rows, sup_buf[...], preferred_element_type=jnp.float32)
        shared_hidden[...] = (jax.nn.silu(gate_val) * up_val).astype(jnp.bfloat16)

    def down_unit(turn, unit):
        if turn == 0 and unit == 0:
            for i in range(2 * local + 2, len(pairs)):
                weight_loads[i].wait()
                swaps[i].wait_recv()
        count = width // 4
        cols = slice(unit * count, (unit + 1) * count)
        down_w = down_buf[:, :, :, cols].reshape(local * span, count)
        for piece in range(2):
            result = jnp.dot(
                hidden_buf[piece * 2 * tok : (piece + 1) * 2 * tok, :],
                down_w,
                preferred_element_type=jnp.float32,
            )
            if turn == 0 and piece == 0:
                result = result + jnp.dot(
                    shared_hidden[...], sdown_buf[:, cols], preferred_element_type=jnp.float32
                )
            first = turn * 4 + 2 * piece
            sums_buf[first : first + 2, :, cols] = result.astype(jnp.bfloat16).reshape(2, tok, count)

    mix_rows = mix_in.shape[0]
    group = width // len(WINDOWS)
    halo_copy = remote(
        normed_buf.at[pl.ds(mix_rows, HALO)],
        normed_buf.at[pl.ds(0, HALO)],
        halo_send,
        halo_recv,
        at_flat(my_flat + 1),
    )

    def mix_unit(index):
        if index == 0:
            mix_load.wait()
            norm_rows(mix_buf, mix_gain, normed_buf, mix_rows, HALO)
            go(halo_copy)
            return
        g = index - 1
        window = WINDOWS[g]
        cols = slice(g * group, (g + 1) * group)
        if g == 0:
            halo_copy.wait_recv()
            pool_load.wait()
        rows = 64
        for chunk in range(mix_rows // rows):
            joined = normed_buf[chunk * rows : chunk * rows + rows + HALO, cols].astype(jnp.float32)
            if chunk == 0:
                line = lax.broadcasted_iota(jnp.int32, joined.shape, 0)
                joined = jnp.where((line >= HALO) | (my_flat > 0), joined, 0.0)
            total, reach = joined, 1
            while reach < window:
                total = total + pltpu.roll(total, reach, 0)
                reach *= 2
            position = (
                my_flat * mix_rows
                + chunk * rows
                + lax.broadcasted_iota(jnp.int32, (rows, group), 0)
            )
            taken = jnp.minimum(position + 1, window).astype(jnp.float32)
            pooled = total[HALO:] / taken
            diff_buf[chunk * rows : (chunk + 1) * rows, :] = (pooled - joined[HALO:]).astype(
                jnp.bfloat16
            )
        mixed = jnp.dot(diff_buf[...], pool_buf[g], preferred_element_type=jnp.float32)
        mix_out[:, cols] = (mixed * pool_scale[:, cols]).astype(jnp.bfloat16)

    seen = {}
    for kind, first, second in steps:
        if kind == "gather_send":
            go(gather_copy(first, second))
        elif kind == "gather_wait":
            gather_copy(first, second).wait_recv()
        elif kind == "reduce_send":
            go(reduce_copy(first, second))
        elif kind == "reduce_add":
            reduce_copy(first, second).wait_recv()
            start, count, _ = parts[first]
            goes = reduce_to[first, second][1]
            cols = slice(start, start + count)
            total = sums_buf[flat(goes), :, cols].astype(jnp.float32) + land_buf[
                flat(second), :, cols
            ].astype(jnp.float32)
            seen[first, goes] = seen.get((first, goes), 0) + 1
            if flat(goes) == 0 and seen[first, goes] == len(feeds[first, goes]):
                moe_out[:, cols] = total.astype(jnp.bfloat16)
            else:
                sums_buf[flat(goes), :, cols] = total.astype(jnp.bfloat16)
        elif kind == "unit":
            if second < 2 * local:
                hidden_unit(first, second)
                if first == 0 and second == 2 * local - 1:
                    shared_unit()
            else:
                down_unit(first, second - 2 * local)
        else:
            mix_unit(first)
    for copy in started:
        copy.wait_send()


def sizes_parts(width):
    lanes = width // 128
    shares = ((6, "zyx"), (6, "zxy"), (10, "xzy"), (10, "yzx"))
    parts, start, given = [], 0, 0
    for count, order in shares:
        given += count
        stop = lanes * given // 32 * 128
        if stop > start:
            parts.append((start, stop - start, order))
        start = stop
    return parts


def unit_times(local):
    return [1.5] * (2 * local) + [0.75] * 4


def both_in_one_kernel(
    mix_input,
    mix_gain,
    pool_weight,
    pool_scale,
    moe_input,
    moe_gain,
    expert_ids,
    route_score,
    expert_gate,
    expert_up,
    expert_down,
    shared_gate,
    shared_up,
    shared_down,
):
    tok, width = moe_input.shape
    local, _, wide = expert_gate.shape
    swide = shared_gate.shape[1]
    z_count = lax.axis_size("ep") // 2
    count = 4 * z_count
    mix_rows = mix_input.shape[0]
    group = width // len(WINDOWS)
    sizes = (z_count, tok, width, local, wide, swide, expert_ids.shape[1])
    pair_count = 3 * local + 3
    part_count = len(sizes_parts(width))
    any_spec = pl.BlockSpec(memory_space=pl.ANY)
    vmem = pl.BlockSpec(memory_space=pltpu.VMEM)
    bf16, f32 = jnp.bfloat16, jnp.float32
    dma = pltpu.SemaphoreType.DMA
    flops = 2 * count * tok * width * 6 * local * wide + 2 * mix_rows * width * group
    return pl.pallas_call(
        functools.partial(kernel, sizes),
        out_shape=(
            jax.ShapeDtypeStruct(mix_input.shape, bf16),
            jax.ShapeDtypeStruct(moe_input.shape, bf16),
        ),
        in_specs=[
            any_spec,
            vmem,
            any_spec,
            vmem,
            any_spec,
            vmem,
            vmem,
            vmem,
            any_spec,
            any_spec,
            any_spec,
            any_spec,
            any_spec,
            any_spec,
        ],
        out_specs=(vmem, vmem),
        scratch_shapes=[
            pltpu.VMEM((count, tok, width), bf16),
            pltpu.VMEM((count, tok, width), bf16),
            pltpu.VMEM((count, tok, width), bf16),
            pltpu.VMEM((128, tok), f32),
            pltpu.VMEM((128, tok), f32),
            pltpu.VMEM((tok, 128), f32),
            pltpu.VMEM((local, 2, width, wide), bf16),
            pltpu.VMEM((local, 2, width, wide), bf16),
            pltpu.VMEM((local, 2, wide, width), bf16),
            pltpu.VMEM((width, 2 * swide), bf16),
            pltpu.VMEM((width, 2 * swide), bf16),
            pltpu.VMEM((2 * swide, width), bf16),
            pltpu.VMEM((4 * tok, 2 * local * wide), bf16),
            pltpu.VMEM((2 * tok, 2 * swide), bf16),
            pltpu.VMEM(moe_input.shape, bf16),
            pltpu.VMEM(mix_input.shape, bf16),
            pltpu.VMEM(pool_weight.shape, bf16),
            pltpu.VMEM((mix_rows + HALO, width), bf16),
            pltpu.VMEM((mix_rows, group), bf16),
            dma((pair_count + 3,)),
            dma((pair_count,)),
            dma((pair_count,)),
            dma((count,)),
            dma((count,)),
            dma((part_count * count,)),
            dma((part_count * count,)),
            dma((part_count * count,)),
            dma((part_count * count,)),
            dma,
            dma,
        ],
        compiler_params=pltpu.CompilerParams(
            collective_id=0, has_side_effects=True, vmem_limit_bytes=60 * 1024 * 1024
        ),
        cost_estimate=pl.CostEstimate(flops=flops, bytes_accessed=24 << 20, transcendentals=0),
    )(
        mix_input,
        mix_gain.reshape(1, width),
        pool_weight,
        pool_scale.reshape(1, width),
        moe_input,
        moe_gain.reshape(1, width),
        expert_ids,
        route_score,
        expert_gate,
        expert_up,
        expert_down,
        shared_gate,
        shared_up,
        shared_down,
    )


def mixer(mix_input, mix_gain, pool_weight, pool_scale):
    normed = rms_norm(mix_input, mix_gain)
    row_count, width_all = normed.shape
    reach_rows = max(WINDOWS) - 1
    before = passed_along(normed[row_count - reach_rows :], ("ep", "tp"), 1)
    offset = lax.axis_index(("ep", "tp")) * row_count
    pooled = window_means(normed, before, offset)
    difference = (pooled - normed.astype(jnp.float32).reshape(row_count, len(WINDOWS), -1)).astype(
        jnp.bfloat16
    )
    mixed_out = jnp.einsum(
        "sgc,gcd->sgd", difference, pool_weight, preferred_element_type=jnp.float32
    )
    return (mixed_out.reshape(row_count, width_all) * pool_scale).astype(jnp.bfloat16)


def per_device(
    mix_input,
    mix_gain,
    pool_weight,
    pool_scale,
    moe_input,
    moe_gain,
    expert_ids,
    route_score,
    expert_gate,
    expert_up,
    expert_down,
    shared_gate,
    shared_up,
    shared_down,
):
    ep_count, tp_count = lax.axis_size("ep"), lax.axis_size("tp")
    few_experts = (
        ep_count * expert_gate.shape[0] <= 8 * expert_ids.shape[1]
        and ep_count % 2 == 0
        and 2 < ep_count <= 8
        and tp_count == 4
    )
    if few_experts:
        return both_in_one_kernel(
            mix_input,
            mix_gain,
            pool_weight,
            pool_scale,
            moe_input,
            moe_gain,
            expert_ids,
            route_score,
            expert_gate,
            expert_up,
            expert_down,
            shared_gate,
            shared_up,
            shared_down,
        )
    mix_output = mixer(mix_input, mix_gain, pool_weight, pool_scale)
    h_moe = rms_norm(moe_input, moe_gain)
    route_w = route_score / jnp.sum(route_score, axis=1, keepdims=True) * ROUTED_SCALE
    moe_output = routed_by_slots(
        h_moe,
        expert_ids,
        route_w,
        expert_gate,
        expert_up,
        expert_down,
        shared_gate,
        shared_up,
        shared_down,
    )
    return (mix_output, moe_output)


def solution(mesh):
    return jax.shard_map(
        per_device,
        mesh=mesh,
        in_specs=(
            P(("ep", "tp"), None),
            P(),
            P(),
            P(),
            P(("ep", "tp"), None),
            P(),
            P("ep", None),
            P(("ep", "tp"), None),
            P("ep", None, "tp"),
            P("ep", None, "tp"),
            P("ep", "tp", None),
            P(None, "tp"),
            P(None, "tp"),
            P("tp", None),
        ),
        out_specs=(P(("ep", "tp"), None), P(("ep", "tp"), None)),
        check_vma=False,
    )
```

```python
import functools

import jax
import jax.numpy as jnp
from jax import lax
from jax.experimental import pallas as pl
from jax.experimental.pallas import tpu as pltpu
from jax.sharding import PartitionSpec as P

WINDOWS = (2, 4, 8, 16)
RMS_EPS = 1e-06
ROUTED_SCALE = 2.5


def passed_along(value, axis, by):
    length = lax.axis_size(axis)
    pairs = [(i, i + by) for i in range(length) if 0 <= i + by < length]
    return lax.ppermute(value, axis, pairs)


def rms_norm(values, gain_row):
    upcast = values.astype(jnp.float32)
    scaled = upcast * lax.rsqrt(jnp.mean(upcast * upcast, axis=-1, keepdims=True) + RMS_EPS)
    return (scaled * gain_row).astype(jnp.bfloat16)


def rounded(values):
    return lax.optimization_barrier(values.astype(jnp.bfloat16)).astype(jnp.float32)


def window_means(normed, before, offset):
    row_count = normed.shape[0]
    lead_rows = before.shape[0]
    group_size = normed.shape[1] // len(WINDOWS)
    joined = jnp.concatenate([before, normed], axis=0).astype(jnp.float32)
    positions = offset + jnp.arange(row_count, dtype=jnp.int32)
    window_avg = []
    for group_idx, span in enumerate(WINDOWS):
        channels = joined[:, group_idx * group_size : (group_idx + 1) * group_size]
        first_row = lead_rows - span + 1
        running = channels[first_row : first_row + row_count]
        for shift_idx in range(1, span):
            running = running + channels[first_row + shift_idx : first_row + shift_idx + row_count]
        counts = jnp.minimum(positions + 1, span).astype(jnp.float32)
        window_avg.append(running / counts[:, None])
    return jnp.stack(window_avg, axis=1)


def fill_slots(normed, picks, expert_count, capacity):
    tok_count, top_count = picks.shape
    pair_count = tok_count * top_count
    flat_ids = picks.reshape(pair_count)
    matches = flat_ids[:, None] == jnp.arange(expert_count, dtype=jnp.int32)[None, :]
    pair_line = jnp.arange(pair_count, dtype=jnp.int32)
    lower_mask = (pair_line[:, None] > pair_line[None, :]).astype(jnp.bfloat16)
    seen_before = jnp.dot(
        lower_mask, matches.astype(jnp.bfloat16), preferred_element_type=jnp.float32
    )
    rank = jnp.sum(seen_before * matches.astype(jnp.float32), axis=1).astype(jnp.int32)
    slots = flat_ids * capacity + rank
    owner = pair_line // top_count
    slot_token = jnp.full((expert_count * capacity,), tok_count, jnp.int32).at[slots].set(owner)
    padded = jnp.concatenate([normed, jnp.zeros((1, normed.shape[1]), normed.dtype)], axis=0)
    return (padded[slot_token], slots.reshape(tok_count, top_count))


def blockwise_down(hidden, down_rows, pieces, contract):
    block_width = hidden.shape[-1] // pieces
    summed = None
    for part_idx in range(pieces):
        piece_out = jnp.einsum(
            contract,
            hidden[..., part_idx * block_width : (part_idx + 1) * block_width],
            down_rows[..., part_idx * block_width : (part_idx + 1) * block_width, :],
            preferred_element_type=jnp.float32,
        )
        summed = rounded(piece_out) if summed is None else summed + rounded(piece_out)
    return summed.astype(jnp.bfloat16)


def routed_by_slots(h_moe, expert_ids, route_w, expert_gate, expert_up, expert_down, shared_gate, shared_up, shared_down):
    tok_count, model_width = h_moe.shape
    top_count = expert_ids.shape[1]
    quarters = lax.axis_size("tp")
    my_quarter = lax.axis_index("tp")
    ep_count = lax.axis_size("ep")
    local_experts = expert_gate.shape[0]
    expert_count = ep_count * local_experts
    capacity = 3 * tok_count * top_count // (2 * expert_count)
    per_source = local_experts * capacity
    full_gate, full_up, full_down, full_sgate, full_sup, full_sdown = (
        lax.all_gather(expert_gate, "tp", axis=2, tiled=True),
        lax.all_gather(expert_up, "tp", axis=2, tiled=True),
        lax.all_gather(expert_down, "tp", axis=1, tiled=True),
        lax.all_gather(shared_gate, "tp", axis=1, tiled=True),
        lax.all_gather(shared_up, "tp", axis=1, tiled=True),
        lax.all_gather(shared_down, "tp", axis=0, tiled=True),
    )
    my_ids = lax.dynamic_slice_in_dim(expert_ids, my_quarter * tok_count, tok_count, 0)
    outgoing, my_slots = fill_slots(h_moe, my_ids, expert_count, capacity)
    landed = lax.all_to_all(
        outgoing.reshape(ep_count, per_source, model_width),
        "ep",
        split_axis=0,
        concat_axis=0,
        tiled=True,
    )
    routed_in = landed.reshape(ep_count, local_experts, capacity, model_width)
    gate_val = jnp.einsum(
        "necd,edf->necf", routed_in, full_gate, preferred_element_type=jnp.float32
    )
    up_val = jnp.einsum("necd,edf->necf", routed_in, full_up, preferred_element_type=jnp.float32)
    hidden = (jax.nn.silu(gate_val) * up_val).astype(jnp.bfloat16)
    expert_back = blockwise_down(hidden, full_down, quarters, "necf,efd->necd")
    expert_back = expert_back.reshape(ep_count, per_source, model_width)
    shared_gate_val = jnp.dot(h_moe, full_sgate, preferred_element_type=jnp.float32)
    shared_up_val = jnp.dot(h_moe, full_sup, preferred_element_type=jnp.float32)
    shared_hidden = (jax.nn.silu(shared_gate_val) * shared_up_val).astype(jnp.bfloat16)
    shared_back = blockwise_down(shared_hidden, full_sdown, quarters, "tf,fd->td")
    returned = lax.all_to_all(expert_back, "ep", split_axis=0, concat_axis=0, tiled=True)
    returned = returned.reshape(expert_count * capacity, model_width)
    combined = shared_back.astype(jnp.float32)
    for pick_idx in range(top_count):
        combined = combined + route_w[:, pick_idx : pick_idx + 1] * returned[
            my_slots[:, pick_idx]
        ].astype(jnp.float32)
    return combined.astype(jnp.bfloat16)


HALO = 16


def flat(dz, dy, dx):
    return dz * 4 + dy * 2 + dx


def build_tasks(parts, z_count, turns, units, block_us, cap_share):
    tasks = {}
    total = sum(part[1] for part in parts)

    def message(name, link, rows, needs):
        tasks[name] = (needs, link, block_us * parts[name[1]][1] / total * rows)

    def local(name, cost, needs):
        tasks[name] = (needs, None, cost)

    last = z_count - 1
    computed = {dz: ("unit", dz, len(units) - 1) for dz in range(z_count)}
    for p, (_, columns, order) in enumerate(parts):
        scale = columns / total
        wide_x = order == "xzy"
        message(("fx", p), "x", 1.0, [])
        for dz in range(z_count):
            for dx in range(2):
                if dx and dz and not wide_x:
                    continue
                if dz:
                    before = ("fz", p, dz - 1, dx) if dz > 1 else ("fx", p)
                    message(("fz", p, dz, dx), "z", 1.0, [before] if dz > 1 or dx else [])
                    held = [("fz", p, dz, dx)]
                else:
                    held = [("fx", p)] if dx else []
                local(("pack", p, dz, dx), 1.2 * scale + 0.1, held)
                ends = [computed[dz]]
                if not dx or wide_x:
                    message(("gy", p, dz, dx), "y", cap_share, [("pack", p, dz, dx)])
                    sums = [computed[dz]] if wide_x else [("addx", p, dz, 1)]
                    message(("ry", p, dz, dx), "y", cap_share, sums)
                    ends.append(("ry", p, dz, dx))
                    if dz > 1:
                        ends.append(("rz", p, dz - 1, dx))
                    elif dz == 0:
                        ends.append(("rz", p, last, dx))
                if not wide_x and not dx and dz:
                    ends.append(("addx", p, dz, 0))
                if not dz and not dx:
                    ends.append(("rfx", p))
                local(("open", p, dz, dx), 1.6 * scale + 0.1, ends)
                if dz:
                    message(("rz", p, dz, dx), "z", 1.0, [("open", p, dz, dx)])
                elif dx:
                    message(("rfx", p), "x", 1.0, [("open", p, 0, 1)])
            if not wide_x:
                for dy in range(2):
                    if dz or dy:
                        source = ("gy", p, dz, 0) if dy else ("pack", p, dz, 0)
                        message(("gx", p, dz, dy), "x", cap_share, [source])
                        message(("rx", p, dz, dy), "x", cap_share, [computed[dz]])
                        local(("addx", p, dz, dy), 0.6 * scale + 0.05, [("rx", p, dz, dy)])
                        tasks["addx", p, dz, dy][0].append(computed[dz])
    before = None
    for dz in turns:
        needs = []
        for p, (_, _, order) in enumerate(parts):
            wide_x = order == "xzy"
            needs += [("pack", p, dz, 0), ("gy", p, dz, 0)]
            if wide_x:
                needs += [("pack", p, dz, 1), ("gy", p, dz, 1)]
            else:
                needs += [("gx", p, dz, 1), ("gx", p, dz, 0) if dz else ("pack", p, 0, 1)]
        for u, cost in enumerate(units):
            local(("unit", dz, u), cost, ([before] if before else []) + (needs if u == 0 else []))
            before = ("unit", dz, u)
    return tasks


def plan_steps(tasks, mixes, delay=2.3):
    after = {}
    for name, (needs, _, _) in tasks.items():
        for need in needs:
            after.setdefault(need, []).append(name)
    tail = {}

    def path(name):
        if name not in tail:
            _, link, cost = tasks[name]
            rest = max([path(q) for q in after.get(name, [])], default=0.0)
            tail[name] = cost + (delay if link else 0.0) + rest
        return tail[name]

    rank = sorted(tasks, key=lambda name: (-path(name), str(name)))
    clock, steps, done, started = 3.0, [], {}, set()
    free = {"x": 0.0, "y": 0.0, "z": 0.0}
    mixed = 0
    while len(started) < len(tasks):
        ready = [
            name
            for name in rank
            if name not in started
            and all(done.get(need, 1e9) <= clock for need in tasks[name][0])
        ]
        sends = [name for name in ready if tasks[name][1]]
        if sends:
            name = sends[0]
            _, link, cost = tasks[name]
            free[link] = max(clock, free[link]) + cost
            done[name] = free[link] + delay
            started.add(name)
            steps.append(name)
        elif ready:
            clock += tasks[ready[0]][2]
            done[ready[0]] = clock
            started.add(ready[0])
            steps.append(ready[0])
        else:
            arrival = min(t for t in done.values() if t > clock)
            if mixed < mixes and arrival - clock > 0.3:
                steps.append(("mix", mixed))
                mixed += 1
                clock += 1.2
            else:
                clock = arrival
    steps.extend(("mix", i) for i in range(mixed, mixes))
    return steps, clock


def norm_rows(source, gain_ref, target, row_count, target_row):
    rows = 32

    def one(i, _):
        start = pl.multiple_of(i * rows, rows)
        upcast = source[pl.ds(start, rows), :].astype(jnp.float32)
        scaled = upcast * lax.rsqrt(jnp.mean(upcast * upcast, axis=-1, keepdims=True) + RMS_EPS)
        goes = pl.multiple_of(start + target_row, 16)
        target[pl.ds(goes, rows), :] = (scaled * gain_ref[...]).astype(jnp.bfloat16)
        return 0

    lax.fori_loop(0, row_count // rows, one, 0)


def kernel(
    sizes,
    mix_in,
    mix_gain,
    pool_w,
    pool_scale,
    moe_in,
    moe_gain,
    ids_ref,
    score_ref,
    gate_in,
    up_in,
    down_in,
    sgate_in,
    sup_in,
    sdown_in,
    mix_out,
    moe_out,
    full_buf,
    packed_buf,
    packed_y,
    result_buf,
    result_land,
    sums_buf,
    sums_land,
    share_own,
    share_all,
    rank_buf,
    before_buf,
    pick_buf,
    place_buf,
    slot_weight,
    gate_buf,
    up_buf,
    down_buf,
    sgate_buf,
    sup_buf,
    sdown_buf,
    hidden_buf,
    shared_hidden,
    moe_buf,
    mix_buf,
    pool_buf,
    normed_buf,
    diff_buf,
    local_sem,
    swap_send,
    swap_recv,
    share_send,
    share_recv,
    block_send,
    block_recv,
    halo_send,
    halo_recv,
):
    z_count, tok, width, local, wide, swide, top, cap = sizes
    ep_count, tp_count = 2 * z_count, 4
    my_ep, my_tp = lax.axis_index("ep"), lax.axis_index("tp")
    my_z, my_y, my_x, my_core = my_ep // 2, my_ep % 2, my_tp // 2, my_tp % 2
    partner = (my_ep, my_x * 2 + (1 - my_core))
    device_count = ep_count * tp_count
    my_flat = my_ep * tp_count + my_tp
    blocks = [(dz, dy, dx) for dz in range(z_count) for dy in range(2) for dx in range(2)]
    bf16, f32 = jnp.bfloat16, jnp.float32

    def spot(dz, dy, dx):
        z = (my_z + dz) % z_count
        y = (my_y + dy) % 2
        x = (my_x + dx) % 2
        return (z * 2 + y, x * 2 + my_core)

    def at_flat(index):
        index = (index + device_count) % device_count
        return (index // tp_count, index % tp_count)

    loads = []

    def load(source, target):
        copy = pltpu.make_async_copy(source, target, local_sem.at[len(loads)])
        copy.start()
        loads.append(copy)
        return copy

    moe_load = load(moe_in, moe_buf)
    mix_load = load(mix_in, mix_buf)
    pairs = []
    for e in range(local):
        for source, target in ((gate_in, gate_buf), (up_in, up_buf)):
            pairs.append((source.at[e], target.at[e, 0], target.at[e, 1]))
    pairs.append((sgate_in, sgate_buf.at[:, pl.ds(0, swide)], sgate_buf.at[:, pl.ds(swide, swide)]))
    pairs.append((sup_in, sup_buf.at[:, pl.ds(0, swide)], sup_buf.at[:, pl.ds(swide, swide)]))
    pairs.append((sdown_in, sdown_buf.at[pl.ds(0, swide)], sdown_buf.at[pl.ds(swide, swide)]))
    for e in range(local):
        pairs.append((down_in.at[e], down_buf.at[e, 0], down_buf.at[e, 1]))
    weight_loads = [load(source, own) for source, own, _ in pairs]
    pool_load = load(pool_w, pool_buf)

    barrier = pltpu.get_barrier_semaphore()
    outer = at_flat(my_flat + 2 * my_core - 1)
    peers = [spot(*b) for b in blocks[1:]] + [partner, outer]
    for peer in peers:
        pl.semaphore_signal(barrier, inc=1, device_id=peer, device_id_type=pl.DeviceIdType.MESH)

    rows_of = 2 * z_count * 8
    scores = score_ref[...]
    route_w = scores / jnp.sum(scores, axis=0, keepdims=True) * ROUTED_SCALE
    line = lax.broadcasted_iota(jnp.int32, (rows_of, tok), 0)
    of_y = (my_y + line // (8 * z_count) + line // 4 % 2) % 2
    named = ((line // 8 % z_count) * 2 + of_y) * local + line % 4
    named = jnp.where(line % 4 < local, named, -1)
    share = jnp.zeros((rows_of, tok), f32)
    ids_at = pl.ds(pl.multiple_of(my_tp * tok, tok), tok)
    for pick in range(top):
        share = share + jnp.where(
            ids_ref[pick : pick + 1, ids_at] == named, route_w[pick : pick + 1, :], 0.0
        )
    share_own[...] = share
    share_all[0:8, :] = share_own[pl.ds(pl.multiple_of(my_z * 8, 8), 8), :]
    before_buf[...] = (
        lax.broadcasted_iota(jnp.int32, (tok, tok), 0)
        < lax.broadcasted_iota(jnp.int32, (tok, tok), 1)
    ).astype(f32).astype(bf16)

    moe_load.wait()
    norm_rows(moe_buf, moe_gain, full_buf.at[0], tok, 0)

    pl.semaphore_wait(barrier, len(peers))

    def remote(source, target, send, recv, device):
        return pltpu.make_async_remote_copy(
            src_ref=source,
            dst_ref=target,
            send_sem=send,
            recv_sem=recv,
            device_id=device,
            device_id_type=pl.DeviceIdType.MESH,
        )

    started = []

    def go(copy):
        copy.start()
        started.append(copy)
        return copy

    shares, swaps = {}, []

    def send_shares():
        for b in blocks[1:]:
            row = pl.multiple_of((b[1] * z_count + (my_z + b[0]) % z_count) * 8, 8)
            shares[b] = go(
                remote(
                    share_own.at[pl.ds(row, 8)],
                    share_all.at[pl.ds(flat(*b) * 8, 8)],
                    share_send.at[flat(*b)],
                    share_recv.at[flat(*b)],
                    spot(*b),
                )
            )
        for i, (source, _, other) in enumerate(pairs):
            swaps.append(go(remote(source, other, swap_send.at[i], swap_recv.at[i], partner)))

    parts = column_parts(width)
    steps, _, numbers = plan(z_count, local, tok, width, cap)
    toward = {"z": (1, 0, 0), "y": (0, 1, 0), "x": (0, 0, 1)}
    every = pl.ds(0, local)

    def message(name):
        kind, p = name[0], name[1]
        cols = pl.ds(parts[p][0], parts[p][1])

        def full(buf, dz, dx):
            return buf.at[dz * 2 + dx, :, cols]

        def packed(buf, dz, dy, dx):
            return buf.at[every, flat(dz, dy, dx), :, cols]

        if kind == "fx":
            source, target, link = full(full_buf, 0, 0), full(full_buf, 0, 1), "x"
        elif kind == "fz":
            _, _, dz, dx = name
            source, target, link = full(full_buf, dz - 1, dx), full(full_buf, dz, dx), "z"
        elif kind == "gy":
            _, _, dz, dx = name
            source = packed_y.at[every, dz * 2 + dx, :, cols]
            target, link = packed(packed_buf, dz, 1, dx), "y"
        elif kind == "gx":
            _, _, dz, dy = name
            source, target = packed(packed_buf, dz, dy, 0), packed(packed_buf, dz, dy, 1)
            link = "x"
        elif kind == "rx":
            _, _, dz, dy = name
            source, target = packed(result_buf, dz, dy, 1), packed(result_land, dz, dy, 1)
            link = "x"
        elif kind == "ry":
            _, _, dz, dx = name
            source, target = packed(result_buf, dz, 1, dx), packed(result_land, dz, 1, dx)
            link = "y"
        elif kind == "rz":
            _, _, dz, dx = name
            source, target, link = full(sums_buf, dz, dx), full(sums_land, dz, dx), "z"
        else:
            source, target, link = full(sums_buf, 0, 1), full(sums_land, 0, 1), "x"
        slot = numbers[name]
        return remote(
            source, target, block_send.at[slot], block_recv.at[slot], spot(*toward[link])
        )

    ranked = set()

    def ensure_rank(b):
        if b in ranked:
            return
        ranked.add(b)
        if b in shares:
            shares[b].wait_recv()
        rows = slice(flat(*b) * 8, flat(*b) * 8 + 8)
        chosen = share_all[rows, :] > 0.0
        count = jnp.dot(
            jnp.where(chosen, 1.0, 0.0).astype(bf16), before_buf[...], preferred_element_type=f32
        )
        rank_buf[rows, :] = jnp.where(chosen, count, -1.0)

    def slot_rows(b, e):
        line = flat(*b) * 8 + e
        slots = lax.broadcasted_iota(jnp.int32, (cap, tok), 0).astype(f32)
        return rank_buf[line : line + 1, :] == slots, share_all[line : line + 1, :]

    picked = set()
    lines = list(range(local)) + list(range(4, 4 + local))

    def pack_unit(p, dz, dx):
        b, f = (dz, 0, dx), dz * 2 + dx
        if f not in picked:
            picked.add(f)
            ensure_rank(b)
            for i, e in enumerate(lines):
                hit, _ = slot_rows(b, e)
                pick_buf[f, i * cap : (i + 1) * cap, :] = jnp.where(hit, 1.0, 0.0).astype(bf16)
        cols = slice(parts[p][0], parts[p][0] + parts[p][1])
        taken = lines if ("gy", p, dz, dx) in numbers else lines[:local]
        rows = jnp.dot(
            pick_buf[f, : len(taken) * cap, :], full_buf[f, :, cols], preferred_element_type=f32
        ).astype(bf16)
        for i in range(len(taken)):
            piece = rows[i * cap : (i + 1) * cap]
            if i < local:
                packed_buf[i, flat(*b), :, cols] = piece
            else:
                packed_y[i - local, f, :, cols] = piece

    placed = set()

    def open_unit(p, dz, dx):
        b, f = (dz, 0, dx), dz * 2 + dx
        slots = 2 * local * cap
        if f not in placed:
            placed.add(f)
            turned = rank_buf[flat(*b) * 8 : flat(*b) * 8 + 8, :].T
            lane = lax.broadcasted_iota(jnp.int32, (tok, slots), 1)
            rank = jnp.full((tok, slots), -1.0, f32)
            for i, e in enumerate(lines):
                rank = jnp.where(lane // cap == i, turned[:, e : e + 1], rank)
            hit = rank == (lane % cap).astype(f32)
            place_buf[f, :, :] = jnp.where(hit, 1.0, 0.0).astype(bf16)
        cols = slice(parts[p][0], parts[p][0] + parts[p][1])
        pieces = [result_buf[e, flat(*b), :, cols] for e in range(local)]
        if ("ry", p, dz, dx) in numbers:
            pieces += [result_land[e, flat(dz, 1, dx), :, cols] for e in range(local)]
        values = jnp.concatenate(pieces, axis=0)
        total = jnp.dot(
            place_buf[f, :, : len(pieces) * cap], values, preferred_element_type=f32
        )
        if dz == 0:
            total = total + jnp.dot(
                shared_hidden[dx * tok : (dx + 1) * tok, :],
                sdown_buf[:, cols],
                preferred_element_type=f32,
            )
        before = ("rz", p, dz - 1 if dz else z_count - 1, dx)
        if before in numbers and dz != 1:
            total = total + sums_land[before[2] * 2 + dx, :, cols].astype(f32)
        if dz == 0 and dx == 0:
            total = total + sums_land[1, :, cols].astype(f32)
            moe_out[:, cols] = total.astype(bf16)
        else:
            sums_buf[f, :, cols] = total.astype(bf16)

    def add_unit(p, dz, dy):
        cols = slice(parts[p][0], parts[p][0] + parts[p][1])
        for e in range(local):
            mine = result_buf[e, flat(dz, dy, 0), :, cols].astype(f32)
            other = result_land[e, flat(dz, dy, 1), :, cols].astype(f32)
            result_buf[e, flat(dz, dy, 0), :, cols] = (mine + other).astype(bf16)

    loaded = set()

    def have_weights(i, side):
        if (i, side) not in loaded:
            loaded.add((i, side))
            if side:
                swaps[i].wait_recv()
            else:
                weight_loads[i].wait()

    def hidden_unit(dz, unit):
        e, side = unit // 2, unit % 2
        if unit == 0:
            for at, b in enumerate(blocks[dz * 4 : dz * 4 + 4]):
                ensure_rank(b)
                for i in range(local):
                    hit, weights = slot_rows(b, i)
                    slot_weight[i, at * cap : (at + 1) * cap, :] = jnp.sum(
                        jnp.where(hit, weights, 0.0), axis=1, keepdims=True
                    )
        for i in (2 * e, 2 * e + 1):
            have_weights(i, side)
        rows = packed_buf[e, dz * 4 : dz * 4 + 4].reshape(4 * cap, width)
        gate_val = jnp.dot(rows, gate_buf[e, side], preferred_element_type=f32)
        up_val = jnp.dot(rows, up_buf[e, side], preferred_element_type=f32)
        hidden = jax.nn.silu(gate_val) * up_val * slot_weight[e]
        hidden_buf[e, :, side * wide : (side + 1) * wide] = hidden.astype(bf16)

    def shared_unit():
        for i in range(2 * local, 2 * local + 3):
            have_weights(i, 0)
            have_weights(i, 1)
        rows = full_buf[0:2].reshape(2 * tok, width)
        gate_val = jnp.dot(rows, sgate_buf[...], preferred_element_type=f32)
        up_val = jnp.dot(rows, sup_buf[...], preferred_element_type=f32)
        shared_hidden[...] = (jax.nn.silu(gate_val) * up_val).astype(bf16)

    def down_unit(dz, e):
        for side in range(2):
            have_weights(2 * local + 3 + e, side)
        count = width // 4
        for piece in range(4):
            cols = slice(piece * count, (piece + 1) * count)
            result = jnp.dot(
                hidden_buf[e],
                down_buf[e, :, :, cols].reshape(2 * wide, count),
                preferred_element_type=f32,
            )
            result_buf[e, dz * 4 : dz * 4 + 4, :, cols] = result.astype(bf16).reshape(4, cap, count)

    mix_rows = mix_in.shape[0]
    group = width // len(WINDOWS)
    halo_copy = remote(
        normed_buf.at[pl.ds(mix_rows, HALO)],
        normed_buf.at[pl.ds(0, HALO)],
        halo_send,
        halo_recv,
        at_flat(my_flat + 1),
    )

    def mix_unit(index):
        if index == 0:
            mix_load.wait()
            norm_rows(mix_buf, mix_gain, normed_buf, mix_rows, HALO)
            go(halo_copy)
            return
        g = index - 1
        window = WINDOWS[g]
        cols = slice(g * group, (g + 1) * group)
        if g == 0:
            halo_copy.wait_recv()
            pool_load.wait()
        rows = 64
        for chunk in range(mix_rows // rows):
            joined = normed_buf[chunk * rows : chunk * rows + rows + HALO, cols].astype(f32)
            if chunk == 0:
                line = lax.broadcasted_iota(jnp.int32, joined.shape, 0)
                joined = jnp.where((line >= HALO) | (my_flat > 0), joined, 0.0)
            total, reach = joined, 1
            while reach < window:
                total = total + pltpu.roll(total, reach, 0)
                reach *= 2
            position = (
                my_flat * mix_rows
                + chunk * rows
                + lax.broadcasted_iota(jnp.int32, (rows, group), 0)
            )
            taken = jnp.minimum(position + 1, window).astype(f32)
            pooled = total[HALO:] / taken
            diff_buf[chunk * rows : (chunk + 1) * rows, :] = (pooled - joined[HALO:]).astype(bf16)
        mixed = jnp.dot(diff_buf[...], pool_buf[g], preferred_element_type=f32)
        mix_out[:, cols] = (mixed * pool_scale[:, cols]).astype(bf16)

    waited = set()
    send_shares()
    tasks = plan(z_count, local, tok, width, cap)[1]
    for name in steps:
        for need in tasks[name][0] if name in tasks else ():
            if need in numbers and need not in waited:
                waited.add(need)
                message(need).wait_recv()
        kind = name[0]
        if name in numbers:
            go(message(name))
        elif kind == "pack":
            pack_unit(*name[1:])
        elif kind == "open":
            open_unit(*name[1:])
        elif kind == "addx":
            add_unit(*name[1:])
        elif kind == "mix":
            mix_unit(name[1])
        elif name[2] < 2 * local:
            hidden_unit(name[1], name[2])
            if name[1] == 0 and name[2] == 2 * local - 1:
                shared_unit()
        else:
            down_unit(name[1], name[2] - 2 * local)
    for copy in started:
        copy.wait_send()


def column_parts(width):
    lanes = width // 128
    parts, start, given = [], 0, 0
    for count, order in PARTS:
        given += count
        stop = lanes * given // 16 * 128
        if stop > start:
            parts.append((start, stop - start, order))
        start = stop
    return parts


PARTS = ((5, "zyx"), (5, "zyx"), (3, "xzy"), (3, "xzy"))


@functools.lru_cache
def plan(z_count, local, tok, width, cap):
    turns = tuple(range(1, z_count)) + (0,)
    units = (0.7,) * (2 * local) + (0.7,) * local
    tasks = build_tasks(
        column_parts(width), z_count, turns, units, tok * width * 2 / 46.6e3, local * cap / tok
    )
    steps, _ = plan_steps(tasks, 1 + len(WINDOWS))
    names = [name for name in tasks if tasks[name][1]]
    return steps, tasks, {name: i for i, name in enumerate(names)}


def both_in_one_kernel(
    mix_input,
    mix_gain,
    pool_weight,
    pool_scale,
    moe_input,
    moe_gain,
    expert_ids,
    route_score,
    expert_gate,
    expert_up,
    expert_down,
    shared_gate,
    shared_up,
    shared_down,
):
    tok, width = moe_input.shape
    local, _, wide = expert_gate.shape
    swide = shared_gate.shape[1]
    z_count = lax.axis_size("ep") // 2
    top = expert_ids.shape[1]
    cap = 3 * tok * top // (4 * z_count * local)
    count = 4 * z_count
    mix_rows = mix_input.shape[0]
    group = width // len(WINDOWS)
    sizes = (z_count, tok, width, local, wide, swide, top, cap)
    pair_count = 3 * local + 3
    message_count = len(plan(z_count, local, tok, width, cap)[2])
    any_spec = pl.BlockSpec(memory_space=pl.ANY)
    vmem = pl.BlockSpec(memory_space=pltpu.VMEM)
    bf16, f32 = jnp.bfloat16, jnp.float32
    dma = pltpu.SemaphoreType.DMA
    flops = 2 * count * cap * local * width * 6 * wide + 2 * mix_rows * width * group
    return pl.pallas_call(
        functools.partial(kernel, sizes),
        out_shape=(
            jax.ShapeDtypeStruct(mix_input.shape, bf16),
            jax.ShapeDtypeStruct(moe_input.shape, bf16),
        ),
        in_specs=[
            any_spec,
            vmem,
            any_spec,
            vmem,
            any_spec,
            vmem,
            vmem,
            vmem,
            any_spec,
            any_spec,
            any_spec,
            any_spec,
            any_spec,
            any_spec,
        ],
        out_specs=(vmem, vmem),
        scratch_shapes=[
            pltpu.VMEM((count // 2, tok, width), bf16),
            pltpu.VMEM((local, count, cap, width), bf16),
            pltpu.VMEM((local, count // 2, cap, width), bf16),
            pltpu.VMEM((local, count, cap, width), bf16),
            pltpu.VMEM((local, count, cap, width), bf16),
            pltpu.VMEM((count // 2, tok, width), bf16),
            pltpu.VMEM((count // 2, tok, width), bf16),
            pltpu.VMEM((16 * z_count, tok), f32),
            pltpu.VMEM((8 * count, tok), f32),
            pltpu.VMEM((8 * count, tok), f32),
            pltpu.VMEM((tok, tok), bf16),
            pltpu.VMEM((count // 2, 2 * local * cap, tok), bf16),
            pltpu.VMEM((count // 2, tok, 2 * local * cap), bf16),
            pltpu.VMEM((local, 4 * cap, 1), f32),
            pltpu.VMEM((local, 2, width, wide), bf16),
            pltpu.VMEM((local, 2, width, wide), bf16),
            pltpu.VMEM((local, 2, wide, width), bf16),
            pltpu.VMEM((width, 2 * swide), bf16),
            pltpu.VMEM((width, 2 * swide), bf16),
            pltpu.VMEM((2 * swide, width), bf16),
            pltpu.VMEM((local, 4 * cap, 2 * wide), bf16),
            pltpu.VMEM((2 * tok, 2 * swide), bf16),
            pltpu.VMEM(moe_input.shape, bf16),
            pltpu.VMEM(mix_input.shape, bf16),
            pltpu.VMEM(pool_weight.shape, bf16),
            pltpu.VMEM((mix_rows + HALO, width), bf16),
            pltpu.VMEM((mix_rows, group), bf16),
            dma((pair_count + 3,)),
            dma((pair_count,)),
            dma((pair_count,)),
            dma((count,)),
            dma((count,)),
            dma((message_count,)),
            dma((message_count,)),
            dma,
            dma,
        ],
        compiler_params=pltpu.CompilerParams(
            collective_id=0, has_side_effects=True, vmem_limit_bytes=63 * 1024 * 1024
        ),
        cost_estimate=pl.CostEstimate(flops=flops, bytes_accessed=24 << 20, transcendentals=0),
    )(
        mix_input,
        mix_gain.reshape(1, width),
        pool_weight,
        pool_scale.reshape(1, width),
        moe_input,
        moe_gain.reshape(1, width),
        expert_ids.T,
        route_score.T,
        expert_gate,
        expert_up,
        expert_down,
        shared_gate,
        shared_up,
        shared_down,
    )


def mixer(mix_input, mix_gain, pool_weight, pool_scale):
    normed = rms_norm(mix_input, mix_gain)
    row_count, width_all = normed.shape
    reach_rows = max(WINDOWS) - 1
    before = passed_along(normed[row_count - reach_rows :], ("ep", "tp"), 1)
    offset = lax.axis_index(("ep", "tp")) * row_count
    pooled = window_means(normed, before, offset)
    difference = (pooled - normed.astype(jnp.float32).reshape(row_count, len(WINDOWS), -1)).astype(
        jnp.bfloat16
    )
    mixed_out = jnp.einsum(
        "sgc,gcd->sgd", difference, pool_weight, preferred_element_type=jnp.float32
    )
    return (mixed_out.reshape(row_count, width_all) * pool_scale).astype(jnp.bfloat16)


def per_device(
    mix_input,
    mix_gain,
    pool_weight,
    pool_scale,
    moe_input,
    moe_gain,
    expert_ids,
    route_score,
    expert_gate,
    expert_up,
    expert_down,
    shared_gate,
    shared_up,
    shared_down,
):
    ep_count, tp_count = lax.axis_size("ep"), lax.axis_size("tp")
    few_experts = (
        ep_count * expert_gate.shape[0] <= 8 * expert_ids.shape[1]
        and ep_count % 2 == 0
        and 2 < ep_count <= 8
        and tp_count == 4
        and expert_gate.shape[0] <= 4
    )
    if few_experts:
        return both_in_one_kernel(
            mix_input,
            mix_gain,
            pool_weight,
            pool_scale,
            moe_input,
            moe_gain,
            expert_ids,
            route_score,
            expert_gate,
            expert_up,
            expert_down,
            shared_gate,
            shared_up,
            shared_down,
        )
    mix_output = mixer(mix_input, mix_gain, pool_weight, pool_scale)
    h_moe = rms_norm(moe_input, moe_gain)
    route_w = route_score / jnp.sum(route_score, axis=1, keepdims=True) * ROUTED_SCALE
    moe_output = routed_by_slots(
        h_moe,
        expert_ids,
        route_w,
        expert_gate,
        expert_up,
        expert_down,
        shared_gate,
        shared_up,
        shared_down,
    )
    return (mix_output, moe_output)


def solution(mesh):
    return jax.shard_map(
        per_device,
        mesh=mesh,
        in_specs=(
            P(("ep", "tp"), None),
            P(),
            P(),
            P(),
            P(("ep", "tp"), None),
            P(),
            P("ep", None),
            P(("ep", "tp"), None),
            P("ep", None, "tp"),
            P("ep", None, "tp"),
            P("ep", "tp", None),
            P(None, "tp"),
            P(None, "tp"),
            P("tp", None),
        ),
        out_specs=(P(("ep", "tp"), None), P(("ep", "tp"), None)),
        check_vma=False,
    )
```

```python
import functools

import jax
import jax.numpy as jnp
from jax import lax
from jax.experimental import pallas as pl
from jax.experimental.pallas import tpu as pltpu
from jax.sharding import PartitionSpec as P

WINDOWS = (2, 4, 8, 16)
RMS_EPS = 1e-06
ROUTED_SCALE = 2.5


def passed_along(value, axis, by):
    length = lax.axis_size(axis)
    pairs = [(i, i + by) for i in range(length) if 0 <= i + by < length]
    return lax.ppermute(value, axis, pairs)


def rms_norm(values, gain_row):
    upcast = values.astype(jnp.float32)
    scaled = upcast * lax.rsqrt(jnp.mean(upcast * upcast, axis=-1, keepdims=True) + RMS_EPS)
    return (scaled * gain_row).astype(jnp.bfloat16)


def rounded(values):
    return lax.optimization_barrier(values.astype(jnp.bfloat16)).astype(jnp.float32)


def window_means(normed, before, offset):
    row_count = normed.shape[0]
    lead_rows = before.shape[0]
    group_size = normed.shape[1] // len(WINDOWS)
    joined = jnp.concatenate([before, normed], axis=0).astype(jnp.float32)
    positions = offset + jnp.arange(row_count, dtype=jnp.int32)
    window_avg = []
    for group_idx, span in enumerate(WINDOWS):
        channels = joined[:, group_idx * group_size : (group_idx + 1) * group_size]
        first_row = lead_rows - span + 1
        running = channels[first_row : first_row + row_count]
        for shift_idx in range(1, span):
            running = running + channels[first_row + shift_idx : first_row + shift_idx + row_count]
        counts = jnp.minimum(positions + 1, span).astype(jnp.float32)
        window_avg.append(running / counts[:, None])
    return jnp.stack(window_avg, axis=1)


def fill_slots(normed, picks, expert_count, capacity):
    tok_count, top_count = picks.shape
    pair_count = tok_count * top_count
    flat_ids = picks.reshape(pair_count)
    matches = flat_ids[:, None] == jnp.arange(expert_count, dtype=jnp.int32)[None, :]
    pair_line = jnp.arange(pair_count, dtype=jnp.int32)
    lower_mask = (pair_line[:, None] > pair_line[None, :]).astype(jnp.bfloat16)
    seen_before = jnp.dot(
        lower_mask, matches.astype(jnp.bfloat16), preferred_element_type=jnp.float32
    )
    rank = jnp.sum(seen_before * matches.astype(jnp.float32), axis=1).astype(jnp.int32)
    slots = flat_ids * capacity + rank
    owner = pair_line // top_count
    slot_token = jnp.full((expert_count * capacity,), tok_count, jnp.int32).at[slots].set(owner)
    padded = jnp.concatenate([normed, jnp.zeros((1, normed.shape[1]), normed.dtype)], axis=0)
    return (padded[slot_token], slots.reshape(tok_count, top_count))


def blockwise_down(hidden, down_rows, pieces, contract):
    block_width = hidden.shape[-1] // pieces
    summed = None
    for part_idx in range(pieces):
        piece_out = jnp.einsum(
            contract,
            hidden[..., part_idx * block_width : (part_idx + 1) * block_width],
            down_rows[..., part_idx * block_width : (part_idx + 1) * block_width, :],
            preferred_element_type=jnp.float32,
        )
        summed = rounded(piece_out) if summed is None else summed + rounded(piece_out)
    return summed.astype(jnp.bfloat16)


def routed_by_slots(h_moe, expert_ids, route_w, expert_gate, expert_up, expert_down, shared_gate, shared_up, shared_down):
    tok_count, model_width = h_moe.shape
    top_count = expert_ids.shape[1]
    quarters = lax.axis_size("tp")
    my_quarter = lax.axis_index("tp")
    ep_count = lax.axis_size("ep")
    local_experts = expert_gate.shape[0]
    expert_count = ep_count * local_experts
    capacity = 3 * tok_count * top_count // (2 * expert_count)
    per_source = local_experts * capacity
    full_gate, full_up, full_down, full_sgate, full_sup, full_sdown = (
        lax.all_gather(expert_gate, "tp", axis=2, tiled=True),
        lax.all_gather(expert_up, "tp", axis=2, tiled=True),
        lax.all_gather(expert_down, "tp", axis=1, tiled=True),
        lax.all_gather(shared_gate, "tp", axis=1, tiled=True),
        lax.all_gather(shared_up, "tp", axis=1, tiled=True),
        lax.all_gather(shared_down, "tp", axis=0, tiled=True),
    )
    my_ids = lax.dynamic_slice_in_dim(expert_ids, my_quarter * tok_count, tok_count, 0)
    outgoing, my_slots = fill_slots(h_moe, my_ids, expert_count, capacity)
    landed = lax.all_to_all(
        outgoing.reshape(ep_count, per_source, model_width),
        "ep",
        split_axis=0,
        concat_axis=0,
        tiled=True,
    )
    routed_in = landed.reshape(ep_count, local_experts, capacity, model_width)
    gate_val = jnp.einsum(
        "necd,edf->necf", routed_in, full_gate, preferred_element_type=jnp.float32
    )
    up_val = jnp.einsum("necd,edf->necf", routed_in, full_up, preferred_element_type=jnp.float32)
    hidden = (jax.nn.silu(gate_val) * up_val).astype(jnp.bfloat16)
    expert_back = blockwise_down(hidden, full_down, quarters, "necf,efd->necd")
    expert_back = expert_back.reshape(ep_count, per_source, model_width)
    shared_gate_val = jnp.dot(h_moe, full_sgate, preferred_element_type=jnp.float32)
    shared_up_val = jnp.dot(h_moe, full_sup, preferred_element_type=jnp.float32)
    shared_hidden = (jax.nn.silu(shared_gate_val) * shared_up_val).astype(jnp.bfloat16)
    shared_back = blockwise_down(shared_hidden, full_sdown, quarters, "tf,fd->td")
    returned = lax.all_to_all(expert_back, "ep", split_axis=0, concat_axis=0, tiled=True)
    returned = returned.reshape(expert_count * capacity, model_width)
    combined = shared_back.astype(jnp.float32)
    for pick_idx in range(top_count):
        combined = combined + route_w[:, pick_idx : pick_idx + 1] * returned[
            my_slots[:, pick_idx]
        ].astype(jnp.float32)
    return combined.astype(jnp.bfloat16)


HALO = 16


def flat(dz, dy, dx):
    return dz * 4 + dy * 2 + dx


def build_tasks(gather_parts, reduce_parts, z_count, turns, units, block_us, cap_share):
    tasks = {}
    total = sum(part[1] for part in gather_parts)
    last = z_count - 1
    computed = {dz: ("unit", dz, len(units) - 1) for dz in range(z_count)}
    first_needs = {dz: [] for dz in range(z_count)}

    def local(name, cost, needs):
        tasks[name] = (needs, None, cost)

    for dz in range(z_count):
        for dx in range(2):
            if dz or dx:
                before = ("sz", 0, dz - 1, dx)
                link = "z" if dz else "x"
                needs = [before] if before in tasks else []
                tasks["sz", 0, dz, dx] = (needs, link, SHARE_US)
                first_needs[dz].append(("sz", 0, dz, dx))
            needs = [("sz", 0, dz, dx)] if dz or dx else []
            tasks["sy", 0, dz, dx] = (needs, "y", SHARE_US)
            first_needs[dz].append(("sy", 0, dz, dx))

    for p, (_, columns, order) in enumerate(gather_parts):
        scale = columns / total
        wide_x = order == "xzy"

        def message(name, link, rows, needs):
            tasks[name] = (needs, link, block_us * scale * rows)

        message(("fx", p), "x", 1.0, [])
        for dz in range(z_count):
            for dx in range(2):
                if dx and dz and not wide_x:
                    continue
                if dz:
                    before = ("fz", p, dz - 1, dx) if dz > 1 else ("fx", p)
                    message(("fz", p, dz, dx), "z", 1.0, [before] if dz > 1 or dx else [])
                    held = [("fz", p, dz, dx)]
                else:
                    held = [("fx", p)] if dx else []
                if dz or dx:
                    held.append(("sz", 0, dz, dx))
                local(("pack", p, dz, dx), 0.8 * scale + 0.1, held)
                first_needs[dz].append(("pack", p, dz, dx))
                if not dx or wide_x:
                    message(("gy", p, dz, dx), "y", cap_share, [("pack", p, dz, dx)])
                    first_needs[dz].append(("gy", p, dz, dx))
            if not wide_x:
                for dy in range(2):
                    if dz or dy:
                        source = ("gy", p, dz, 0) if dy else ("pack", p, dz, 0)
                        message(("gx", p, dz, dy), "x", cap_share, [source])
                        first_needs[dz].append(("gx", p, dz, dy))

    for p, (_, columns, order) in enumerate(reduce_parts):
        scale = columns / total
        wide_x = order == "xzy"

        def message(name, link, rows, needs):
            tasks[name] = (needs, link, block_us * scale * rows)

        for dz in range(z_count):
            for dx in range(2):
                if dx and dz and not wide_x:
                    continue
                ends = [computed[dz]]
                if not dx or wide_x:
                    sums = [computed[dz]] if wide_x else [("addx", p, dz, 1)]
                    message(("ry", p, dz, dx), "y", cap_share, sums)
                    ends.append(("ry", p, dz, dx))
                    if dz > 1:
                        ends.append(("rz", p, dz - 1, dx))
                    elif dz == 0:
                        ends.append(("rz", p, last, dx))
                if not wide_x and not dx and dz:
                    ends.append(("addx", p, dz, 0))
                if not dz and not dx:
                    ends.append(("rfx", p))
                local(("open", p, dz, dx), 1.0 * scale + 0.1, ends)
                if dz:
                    message(("rz", p, dz, dx), "z", 1.0, [("open", p, dz, dx)])
                elif dx:
                    message(("rfx", p), "x", 1.0, [("open", p, 0, 1)])
            if not wide_x:
                for dy in range(2):
                    if dz or dy:
                        message(("rx", p, dz, dy), "x", cap_share, [computed[dz]])
                        needs = [("rx", p, dz, dy), computed[dz]]
                        local(("addx", p, dz, dy), 0.4 * scale + 0.05, needs)
    before = None
    for dz in turns:
        for u, cost in enumerate(units):
            needs = first_needs[dz] if u == 0 else []
            local(("unit", dz, u), cost, ([before] if before else []) + needs)
            before = ("unit", dz, u)
    return tasks


def plan_steps(tasks, mixes, delay=2.5):
    after = {}
    for name, (needs, _, _) in tasks.items():
        for need in needs:
            after.setdefault(need, []).append(name)
    tail = {}

    def path(name):
        if name not in tail:
            _, link, cost = tasks[name]
            rest = max([path(q) for q in after.get(name, [])], default=0.0)
            tail[name] = cost + (delay if link else 0.0) + rest
        return tail[name]

    rank = sorted(tasks, key=lambda name: (-path(name) - EARLIER.get(name[0], 0), str(name)))
    clock, steps, done, started = 3.0, [], {}, set()
    free = {"x": 0.0, "y": 0.0, "z": 0.0}
    mixed = 0
    while len(started) < len(tasks):
        ready = [
            name
            for name in rank
            if name not in started
            and all(done.get(need, 1e9) <= clock for need in tasks[name][0])
        ]
        sends = [name for name in ready if tasks[name][1]]
        if sends:
            name = sends[0]
            _, link, cost = tasks[name]
            free[link] = max(clock, free[link]) + cost
            done[name] = free[link] + delay
            started.add(name)
            steps.append(name)
        elif ready:
            clock += tasks[ready[0]][2]
            done[ready[0]] = clock
            started.add(ready[0])
            steps.append(ready[0])
        else:
            arrival = min(t for t in done.values() if t > clock)
            if mixed < mixes and arrival - clock > 0.3:
                steps.append(("mix", mixed))
                mixed += 1
                clock += 1.2
            else:
                clock = arrival
    steps.extend(("mix", i) for i in range(mixed, mixes))
    return steps, clock


def norm_rows(source, gain_ref, target, row_count, target_row):
    rows = 32

    def one(i, _):
        start = pl.multiple_of(i * rows, rows)
        upcast = source[pl.ds(start, rows), :].astype(jnp.float32)
        scaled = upcast * lax.rsqrt(jnp.mean(upcast * upcast, axis=-1, keepdims=True) + RMS_EPS)
        goes = pl.multiple_of(start + target_row, 16)
        target[pl.ds(goes, rows), :] = (scaled * gain_ref[...]).astype(jnp.bfloat16)
        return 0

    lax.fori_loop(0, row_count // rows, one, 0, unroll=4)


def kernel(
    sizes,
    mix_in,
    mix_gain,
    pool_w,
    pool_scale,
    moe_in,
    moe_gain,
    ids_ref,
    score_ref,
    gate_in,
    up_in,
    down_in,
    sgate_in,
    sup_in,
    sdown_in,
    mix_out,
    moe_out,
    full_buf,
    packed_buf,
    packed_y,
    result_buf,
    result_land,
    sums_buf,
    sums_land,
    share_all,
    share_rows,
    rank_buf,
    before_buf,
    pick_buf,
    place_buf,
    slot_weight,
    gate_buf,
    up_buf,
    down_buf,
    sgate_buf,
    sup_buf,
    sdown_buf,
    hidden_buf,
    shared_hidden,
    moe_buf,
    mix_buf,
    pool_buf,
    normed_buf,
    diff_buf,
    local_sem,
    swap_send,
    swap_recv,
    block_send,
    block_recv,
    halo_send,
    halo_recv,
):
    z_count, tok, width, local, wide, swide, top, cap = sizes
    ep_count, tp_count = 2 * z_count, 4
    my_ep, my_tp = lax.axis_index("ep"), lax.axis_index("tp")
    my_z, my_y, my_x, my_core = my_ep // 2, my_ep % 2, my_tp // 2, my_tp % 2
    partner = (my_ep, my_x * 2 + (1 - my_core))
    device_count = ep_count * tp_count
    my_flat = my_ep * tp_count + my_tp
    blocks = [(dz, dy, dx) for dz in range(z_count) for dy in range(2) for dx in range(2)]
    bf16, f32 = jnp.bfloat16, jnp.float32

    def spot(dz, dy, dx):
        z = (my_z + dz) % z_count
        y = (my_y + dy) % 2
        x = (my_x + dx) % 2
        return (z * 2 + y, x * 2 + my_core)

    def at_flat(index):
        index = (index + device_count) % device_count
        return (index // tp_count, index % tp_count)

    loads = []

    def load(source, target):
        copy = pltpu.make_async_copy(source, target, local_sem.at[len(loads)])
        copy.start()
        loads.append(copy)
        return copy

    moe_load = load(moe_in, moe_buf)
    mix_load = load(mix_in, mix_buf)
    pairs = []
    for e in range(local):
        for source, target in ((gate_in, gate_buf), (up_in, up_buf)):
            pairs.append((source.at[e], target.at[e, 0], target.at[e, 1]))
    pairs.append((sgate_in, sgate_buf.at[:, pl.ds(0, swide)], sgate_buf.at[:, pl.ds(swide, swide)]))
    pairs.append((sup_in, sup_buf.at[:, pl.ds(0, swide)], sup_buf.at[:, pl.ds(swide, swide)]))
    pairs.append((sdown_in, sdown_buf.at[pl.ds(0, swide)], sdown_buf.at[pl.ds(swide, swide)]))
    for e in range(local):
        pairs.append((down_in.at[e], down_buf.at[e, 0], down_buf.at[e, 1]))
    weight_loads = [load(source, own) for source, own, _ in pairs]
    pool_load = load(pool_w, pool_buf)

    barrier = pltpu.get_barrier_semaphore()
    outer = at_flat(my_flat + 2 * my_core - 1)
    peers = [spot(1, 0, 0), spot(z_count - 1, 0, 0), spot(0, 1, 0), spot(0, 0, 1), partner]

    def greet(peer):
        pl.semaphore_signal(barrier, inc=1, device_id=peer, device_id_type=pl.DeviceIdType.MESH)

    for peer in peers:
        greet(peer)
    not_first, not_last = my_flat > 0, my_flat < device_count - 1
    has_outer = not_first & not_last

    @pl.when(has_outer)
    def _():
        greet(outer)

    scores = score_ref[...]
    ids_at = pl.ds(pl.multiple_of(my_tp * tok, tok), tok)
    share_all[0, 0:top, :] = ids_ref[:, ids_at].astype(f32)
    share_all[0, 4 : 4 + top, :] = scores / jnp.sum(scores, axis=0, keepdims=True) * ROUTED_SCALE
    line = lax.broadcasted_iota(jnp.int32, (8, tok), 0)
    expert = jnp.where(line < 4, my_ep, my_z * 2 + 1 - my_y) * local + line % 4
    expert = jnp.where(line % 4 < local, expert, -1).astype(f32)
    before_buf[...] = (
        lax.broadcasted_iota(jnp.int32, (tok, tok), 0)
        < lax.broadcasted_iota(jnp.int32, (tok, tok), 1)
    ).astype(f32).astype(bf16)

    moe_load.wait()
    norm_rows(moe_buf, moe_gain, full_buf.at[0], tok, 0)

    pl.semaphore_wait(barrier, len(peers) + has_outer.astype(jnp.int32))

    def remote(source, target, send, recv, device):
        return pltpu.make_async_remote_copy(
            src_ref=source,
            dst_ref=target,
            send_sem=send,
            recv_sem=recv,
            device_id=device,
            device_id_type=pl.DeviceIdType.MESH,
        )

    started = []

    def go(copy):
        copy.start()
        started.append(copy)
        return copy

    swaps = []

    def swap_weights():
        for i, (source, _, other) in enumerate(pairs):
            swaps.append(go(remote(source, other, swap_send.at[i], swap_recv.at[i], partner)))

    gather_parts, reduce_parts = column_parts(width, GATHER), column_parts(width, REDUCE)
    steps, tasks, numbers = plan(z_count, local, tok, width, cap)
    toward = {"z": (1, 0, 0), "y": (0, 1, 0), "x": (0, 0, 1)}
    every = pl.ds(0, local)

    def message(name):
        kind, p = name[0], name[1]
        part = (reduce_parts if kind in ("rx", "rfx", "ry", "rz") else gather_parts)[p]
        cols = pl.ds(part[0], part[1])

        def full(buf, dz, dx):
            return buf.at[dz * 2 + dx, :, cols]

        def packed(buf, dz, dy, dx):
            return buf.at[every, flat(dz, dy, dx), :, cols]

        if kind == "sz":
            _, _, dz, dx = name
            source = share_all.at[flat(dz - 1, 0, dx) if dz else 0]
            target, link = share_all.at[flat(dz, 0, dx)], "z" if dz else "x"
        elif kind == "sy":
            _, _, dz, dx = name
            source, target = share_all.at[flat(dz, 0, dx)], share_all.at[flat(dz, 1, dx)]
            link = "y"
        elif kind == "fx":
            source, target, link = full(full_buf, 0, 0), full(full_buf, 0, 1), "x"
        elif kind == "fz":
            _, _, dz, dx = name
            source, target, link = full(full_buf, dz - 1, dx), full(full_buf, dz, dx), "z"
        elif kind == "gy":
            _, _, dz, dx = name
            source = packed_y.at[every, dz * 2 + dx, :, cols]
            target, link = packed(packed_buf, dz, 1, dx), "y"
        elif kind == "gx":
            _, _, dz, dy = name
            source, target = packed(packed_buf, dz, dy, 0), packed(packed_buf, dz, dy, 1)
            link = "x"
        elif kind == "rx":
            _, _, dz, dy = name
            source, target = packed(result_buf, dz, dy, 1), packed(result_land, dz, dy, 1)
            link = "x"
        elif kind == "ry":
            _, _, dz, dx = name
            source, target = packed(result_buf, dz, 1, dx), packed(result_land, dz, 1, dx)
            link = "y"
        elif kind == "rz":
            _, _, dz, dx = name
            source, target, link = full(sums_buf, dz, dx), full(sums_land, dz, dx), "z"
        else:
            source, target, link = full(sums_buf, 0, 1), full(sums_land, 0, 1), "x"
        return remote(
            source,
            target,
            block_send.at[send_slot[name]],
            block_recv.at[numbers[name]],
            spot(*toward[link]),
        )

    send_slot, in_slot, used = {}, {}, {"x": 0, "y": 0, "z": 0}

    def start_message(name):
        link = tasks[name][1]
        slot = "xyz".index(link) * SEND_SLOTS + used[link] % SEND_SLOTS
        used[link] += 1
        if slot in in_slot:
            message(in_slot[slot]).wait_send()
        send_slot[name], in_slot[slot] = slot, name
        message(name).start()

    ranked = set()
    lines = list(range(local)) + list(range(4, 4 + local))

    def ensure_rank(b):
        if b in ranked:
            return
        ranked.add(b)
        rows = slice(flat(*b) * 8, flat(*b) * 8 + 8)
        chosen, weights = jnp.zeros((8, tok), f32), jnp.zeros((8, tok), f32)
        for pick in range(top):
            hit = share_all[flat(*b), pick : pick + 1, :] == expert
            chosen = jnp.where(hit, 1.0, chosen)
            weights = jnp.where(hit, share_all[flat(*b), 4 + pick : 5 + pick, :], weights)
        share_rows[rows, :] = weights
        count = jnp.dot(chosen.astype(bf16), before_buf[...], preferred_element_type=f32)
        rank_buf[rows, :] = jnp.where(chosen > 0.0, count, -1.0)

    def slot_rows(b, e):
        line = flat(*b) * 8 + e
        slots = lax.broadcasted_iota(jnp.int32, (cap, tok), 0).astype(f32)
        return rank_buf[line : line + 1, :] == slots, share_rows[line : line + 1, :]

    picked = set()

    def pack_unit(p, dz, dx):
        b, f = (dz, 0, dx), dz * 2 + dx
        if f not in picked:
            picked.add(f)
            ensure_rank(b)
            for i, e in enumerate(lines):
                hit, _ = slot_rows(b, e)
                pick_buf[f, i * cap : (i + 1) * cap, :] = jnp.where(hit, 1.0, 0.0).astype(bf16)
        cols = slice(gather_parts[p][0], gather_parts[p][0] + gather_parts[p][1])
        taken = lines if ("gy", p, dz, dx) in numbers else lines[:local]
        rows = jnp.dot(
            pick_buf[f, : len(taken) * cap, :], full_buf[f, :, cols], preferred_element_type=f32
        ).astype(bf16)
        for i in range(len(taken)):
            piece = rows[i * cap : (i + 1) * cap]
            if i < local:
                packed_buf[i, flat(*b), :, cols] = piece
            else:
                packed_y[i - local, f, :, cols] = piece

    placed = set()

    def open_unit(p, dz, dx):
        b, f = (dz, 0, dx), dz * 2 + dx
        slots = 2 * local * cap
        if f not in placed:
            placed.add(f)
            turned = rank_buf[flat(*b) * 8 : flat(*b) * 8 + 8, :].T
            lane = lax.broadcasted_iota(jnp.int32, (tok, slots), 1)
            rank = jnp.full((tok, slots), -1.0, f32)
            for i, e in enumerate(lines):
                rank = jnp.where(lane // cap == i, turned[:, e : e + 1], rank)
            hit = rank == (lane % cap).astype(f32)
            place_buf[f, :, :] = jnp.where(hit, 1.0, 0.0).astype(bf16)
        cols = slice(reduce_parts[p][0], reduce_parts[p][0] + reduce_parts[p][1])
        pieces = [result_buf[e, flat(*b), :, cols] for e in range(local)]
        if ("ry", p, dz, dx) in numbers:
            pieces += [result_land[e, flat(dz, 1, dx), :, cols] for e in range(local)]
        values = jnp.concatenate(pieces, axis=0)
        total = jnp.dot(
            place_buf[f, :, : len(pieces) * cap], values, preferred_element_type=f32
        )
        if dz == 0:
            total = total + jnp.dot(
                shared_hidden[dx * tok : (dx + 1) * tok, :],
                sdown_buf[:, cols],
                preferred_element_type=f32,
            )
        before = ("rz", p, dz - 1 if dz else z_count - 1, dx)
        if before in numbers and dz != 1:
            total = total + sums_land[before[2] * 2 + dx, :, cols].astype(f32)
        if dz == 0 and dx == 0:
            total = total + sums_land[1, :, cols].astype(f32)
            moe_out[:, cols] = total.astype(bf16)
        else:
            sums_buf[f, :, cols] = total.astype(bf16)

    def add_unit(p, dz, dy):
        cols = slice(reduce_parts[p][0], reduce_parts[p][0] + reduce_parts[p][1])
        for e in range(local):
            mine = result_buf[e, flat(dz, dy, 0), :, cols].astype(f32)
            other = result_land[e, flat(dz, dy, 1), :, cols].astype(f32)
            result_buf[e, flat(dz, dy, 0), :, cols] = (mine + other).astype(bf16)

    loaded = set()

    def have_weights(i, side):
        if (i, side) not in loaded:
            loaded.add((i, side))
            if side:
                swaps[i].wait_recv()
            else:
                weight_loads[i].wait()

    def hidden_unit(dz, unit):
        e, side = unit // 2, unit % 2
        if unit == 0:
            for at, b in enumerate(blocks[dz * 4 : dz * 4 + 4]):
                ensure_rank(b)
                for i in range(local):
                    hit, weights = slot_rows(b, i)
                    slot_weight[i, at * cap : (at + 1) * cap, :] = jnp.sum(
                        jnp.where(hit, weights, 0.0), axis=1, keepdims=True
                    )
        for i in (2 * e, 2 * e + 1):
            have_weights(i, side)
        rows = packed_buf[e, dz * 4 : dz * 4 + 4].reshape(4 * cap, width)
        gate_val = jnp.dot(rows, gate_buf[e, side], preferred_element_type=f32)
        up_val = jnp.dot(rows, up_buf[e, side], preferred_element_type=f32)
        hidden = jax.nn.silu(gate_val) * up_val * slot_weight[e]
        hidden_buf[e, :, side * wide : (side + 1) * wide] = hidden.astype(bf16)

    def shared_unit():
        for i in range(2 * local, 2 * local + 3):
            have_weights(i, 0)
            have_weights(i, 1)
        rows = full_buf[0:2].reshape(2 * tok, width)
        gate_val = jnp.dot(rows, sgate_buf[...], preferred_element_type=f32)
        up_val = jnp.dot(rows, sup_buf[...], preferred_element_type=f32)
        shared_hidden[...] = (jax.nn.silu(gate_val) * up_val).astype(bf16)

    def down_unit(dz, e):
        for side in range(2):
            have_weights(2 * local + 3 + e, side)
        count = width // 4
        for piece in range(4):
            cols = slice(piece * count, (piece + 1) * count)
            result = jnp.dot(
                hidden_buf[e],
                down_buf[e, :, :, cols].reshape(2 * wide, count),
                preferred_element_type=f32,
            )
            result_buf[e, dz * 4 : dz * 4 + 4, :, cols] = result.astype(bf16).reshape(4, cap, count)

    mix_rows = mix_in.shape[0]
    group = width // len(WINDOWS)
    halo_copy = remote(
        normed_buf.at[pl.ds(mix_rows, HALO)],
        normed_buf.at[pl.ds(0, HALO)],
        halo_send,
        halo_recv,
        at_flat(my_flat + 1),
    )

    def mix_unit(index):
        if index == 0:
            mix_load.wait()
            norm_rows(mix_buf, mix_gain, normed_buf, mix_rows, HALO)

            @pl.when(not_last)
            def _():
                halo_copy.start()

            return
        g = index - 1
        window = WINDOWS[g]
        cols = slice(g * group, (g + 1) * group)
        if g == 0:
            pool_load.wait()

            @pl.when(not_first)
            def _():
                halo_copy.wait_recv()

        rows = 64
        for chunk in range(mix_rows // rows):
            joined = normed_buf[chunk * rows : chunk * rows + rows + HALO, cols].astype(f32)
            if chunk == 0:
                line = lax.broadcasted_iota(jnp.int32, joined.shape, 0)
                joined = jnp.where((line >= HALO) | (my_flat > 0), joined, 0.0)
            total, reach = joined, 1
            while reach < window:
                total = total + pltpu.roll(total, reach, 0)
                reach *= 2
            position = (
                my_flat * mix_rows
                + chunk * rows
                + lax.broadcasted_iota(jnp.int32, (rows, group), 0)
            )
            taken = jnp.minimum(position + 1, window).astype(f32)
            pooled = total[HALO:] / taken
            diff_buf[chunk * rows : (chunk + 1) * rows, :] = (pooled - joined[HALO:]).astype(bf16)
        mixed = jnp.dot(diff_buf[...], pool_buf[g], preferred_element_type=f32)
        mix_out[:, cols] = (mixed * pool_scale[:, cols]).astype(bf16)

    waited = set()
    for name in steps:
        if not swaps and name not in numbers:
            swap_weights()
        for need in tasks[name][0] if name in tasks else ():
            if need in numbers and need not in waited:
                waited.add(need)
                message(need).wait_recv()
        kind = name[0]
        if name in numbers:
            start_message(name)
        elif kind == "pack":
            pack_unit(*name[1:])
        elif kind == "open":
            open_unit(*name[1:])
        elif kind == "addx":
            add_unit(*name[1:])
        elif kind == "mix":
            mix_unit(name[1])
        elif name[2] < 2 * local:
            hidden_unit(name[1], name[2])
            if name[1] == 0 and name[2] == 2 * local - 1:
                shared_unit()
        else:
            down_unit(name[1], name[2] - 2 * local)
    for copy in started + [message(name) for name in in_slot.values()]:
        copy.wait_send()

    @pl.when(not_last)
    def _():
        halo_copy.wait_send()


def column_parts(width, pattern):
    lanes = width // 128
    parts, start, given = [], 0, 0
    for count, order in pattern:
        given += count
        stop = lanes * given // 16 * 128
        if stop > start:
            parts.append((start, stop - start, order))
        start = stop
    return parts


GATHER = ((5, "zyx"), (5, "zyx"), (3, "xzy"), (3, "xzy"))
REDUCE = ((4, "zyx"), (3, "zyx"), (3, "zyx"), (3, "xzy"), (3, "xzy"))
EARLIER = {"ry": 20, "fx": 5, "sz": 10, "sy": 20, "gy": -10, "rx": -2, "pack": 40, "rz": 5}
EARLIER |= {"rfx": -20, "open": 5, "fz": -5, "gx": 40, "unit": -5}
SHARE_US = 0.09
SEND_SLOTS = 12


@functools.lru_cache
def plan(z_count, local, tok, width, cap):
    turns = tuple(range(1, z_count)) + (0,)
    units = (0.5,) * (3 * local)
    tasks = build_tasks(
        column_parts(width, GATHER),
        column_parts(width, REDUCE),
        z_count,
        turns,
        units,
        tok * width * 2 / 46.6e3,
        local * cap / tok,
    )
    steps, _ = plan_steps(tasks, 1 + len(WINDOWS))
    names = [name for name in tasks if tasks[name][1]]
    return steps, tasks, {name: i for i, name in enumerate(names)}


def both_in_one_kernel(
    mix_input,
    mix_gain,
    pool_weight,
    pool_scale,
    moe_input,
    moe_gain,
    expert_ids,
    route_score,
    expert_gate,
    expert_up,
    expert_down,
    shared_gate,
    shared_up,
    shared_down,
):
    tok, width = moe_input.shape
    local, _, wide = expert_gate.shape
    swide = shared_gate.shape[1]
    z_count = lax.axis_size("ep") // 2
    top = expert_ids.shape[1]
    cap = 3 * tok * top // (4 * z_count * local)
    count = 4 * z_count
    mix_rows = mix_input.shape[0]
    group = width // len(WINDOWS)
    sizes = (z_count, tok, width, local, wide, swide, top, cap)
    pair_count = 3 * local + 3
    message_count = len(plan(z_count, local, tok, width, cap)[2])
    any_spec = pl.BlockSpec(memory_space=pl.ANY)
    vmem = pl.BlockSpec(memory_space=pltpu.VMEM)
    bf16, f32 = jnp.bfloat16, jnp.float32
    dma = pltpu.SemaphoreType.DMA
    flops = 2 * count * cap * local * width * 6 * wide + 2 * mix_rows * width * group
    return pl.pallas_call(
        functools.partial(kernel, sizes),
        out_shape=(pltpu.VMEM(mix_input.shape, bf16), pltpu.VMEM(moe_input.shape, bf16)),
        in_specs=[
            any_spec,
            vmem,
            any_spec,
            vmem,
            any_spec,
            vmem,
            vmem,
            vmem,
            any_spec,
            any_spec,
            any_spec,
            any_spec,
            any_spec,
            any_spec,
        ],
        out_specs=(vmem, vmem),
        scratch_shapes=[
            pltpu.VMEM((count // 2, tok, width), bf16),
            pltpu.VMEM((local, count, cap, width), bf16),
            pltpu.VMEM((local, count // 2, cap, width), bf16),
            pltpu.VMEM((local, count, cap, width), bf16),
            pltpu.VMEM((local, count, cap, width), bf16),
            pltpu.VMEM((count // 2, tok, width), bf16),
            pltpu.VMEM((count // 2, tok, width), bf16),
            pltpu.VMEM((count, 8, tok), f32),
            pltpu.VMEM((8 * count, tok), f32),
            pltpu.VMEM((8 * count, tok), f32),
            pltpu.VMEM((tok, tok), bf16),
            pltpu.VMEM((count // 2, 2 * local * cap, tok), bf16),
            pltpu.VMEM((count // 2, tok, 2 * local * cap), bf16),
            pltpu.VMEM((local, 4 * cap, 1), f32),
            pltpu.VMEM((local, 2, width, wide), bf16),
            pltpu.VMEM((local, 2, width, wide), bf16),
            pltpu.VMEM((local, 2, wide, width), bf16),
            pltpu.VMEM((width, 2 * swide), bf16),
            pltpu.VMEM((width, 2 * swide), bf16),
            pltpu.VMEM((2 * swide, width), bf16),
            pltpu.VMEM((local, 4 * cap, 2 * wide), bf16),
            pltpu.VMEM((2 * tok, 2 * swide), bf16),
            pltpu.VMEM(moe_input.shape, bf16),
            pltpu.VMEM(mix_input.shape, bf16),
            pltpu.VMEM(pool_weight.shape, bf16),
            pltpu.VMEM((mix_rows + HALO, width), bf16),
            pltpu.VMEM((mix_rows, group), bf16),
            dma((pair_count + 3,)),
            dma((pair_count,)),
            dma((pair_count,)),
            dma((3 * SEND_SLOTS,)),
            dma((message_count,)),
            dma,
            dma,
        ],
        compiler_params=pltpu.CompilerParams(
            collective_id=0, has_side_effects=True, vmem_limit_bytes=59 * 1024 * 1024
        ),
        cost_estimate=pl.CostEstimate(flops=flops, bytes_accessed=24 << 20, transcendentals=0),
    )(
        mix_input,
        mix_gain.reshape(1, width),
        pool_weight,
        pool_scale.reshape(1, width),
        moe_input,
        moe_gain.reshape(1, width),
        expert_ids.T,
        route_score.T,
        expert_gate,
        expert_up,
        expert_down,
        shared_gate,
        shared_up,
        shared_down,
    )


def mixer(mix_input, mix_gain, pool_weight, pool_scale):
    normed = rms_norm(mix_input, mix_gain)
    row_count, width_all = normed.shape
    reach_rows = max(WINDOWS) - 1
    before = passed_along(normed[row_count - reach_rows :], ("ep", "tp"), 1)
    offset = lax.axis_index(("ep", "tp")) * row_count
    pooled = window_means(normed, before, offset)
    difference = (pooled - normed.astype(jnp.float32).reshape(row_count, len(WINDOWS), -1)).astype(
        jnp.bfloat16
    )
    mixed_out = jnp.einsum(
        "sgc,gcd->sgd", difference, pool_weight, preferred_element_type=jnp.float32
    )
    return (mixed_out.reshape(row_count, width_all) * pool_scale).astype(jnp.bfloat16)


def per_device(
    mix_input,
    mix_gain,
    pool_weight,
    pool_scale,
    moe_input,
    moe_gain,
    expert_ids,
    route_score,
    expert_gate,
    expert_up,
    expert_down,
    shared_gate,
    shared_up,
    shared_down,
):
    ep_count, tp_count = lax.axis_size("ep"), lax.axis_size("tp")
    few_experts = (
        ep_count * expert_gate.shape[0] <= 8 * expert_ids.shape[1]
        and ep_count % 2 == 0
        and 2 < ep_count <= 8
        and tp_count == 4
        and expert_gate.shape[0] <= 4
        and expert_ids.shape[1] <= 4
    )
    if few_experts:
        return both_in_one_kernel(
            mix_input,
            mix_gain,
            pool_weight,
            pool_scale,
            moe_input,
            moe_gain,
            expert_ids,
            route_score,
            expert_gate,
            expert_up,
            expert_down,
            shared_gate,
            shared_up,
            shared_down,
        )
    mix_output = mixer(mix_input, mix_gain, pool_weight, pool_scale)
    h_moe = rms_norm(moe_input, moe_gain)
    route_w = route_score / jnp.sum(route_score, axis=1, keepdims=True) * ROUTED_SCALE
    moe_output = routed_by_slots(
        h_moe,
        expert_ids,
        route_w,
        expert_gate,
        expert_up,
        expert_down,
        shared_gate,
        shared_up,
        shared_down,
    )
    return (mix_output, moe_output)


def solution(mesh):
    return jax.shard_map(
        per_device,
        mesh=mesh,
        in_specs=(
            P(("ep", "tp"), None),
            P(),
            P(),
            P(),
            P(("ep", "tp"), None),
            P(),
            P("ep", None),
            P(("ep", "tp"), None),
            P("ep", None, "tp"),
            P("ep", None, "tp"),
            P("ep", "tp", None),
            P(None, "tp"),
            P(None, "tp"),
            P("tp", None),
        ),
        out_specs=(P(("ep", "tp"), None), P(("ep", "tp"), None)),
        check_vma=False,
    )
```

```python
import functools

import jax
import jax.numpy as jnp
from jax import lax
from jax.experimental import pallas as pl
from jax.experimental.pallas import tpu as pltpu
from jax.sharding import PartitionSpec as P

WINDOWS = (2, 4, 8, 16)
RMS_EPS = 1e-06
ROUTED_SCALE = 2.5


def passed_along(value, axis, by):
    length = lax.axis_size(axis)
    pairs = [(i, i + by) for i in range(length) if 0 <= i + by < length]
    return lax.ppermute(value, axis, pairs)


def rms_norm(values, gain_row):
    upcast = values.astype(jnp.float32)
    scaled = upcast * lax.rsqrt(jnp.mean(upcast * upcast, axis=-1, keepdims=True) + RMS_EPS)
    return (scaled * gain_row).astype(jnp.bfloat16)


def rounded(values):
    return lax.optimization_barrier(values.astype(jnp.bfloat16)).astype(jnp.float32)


def window_means(normed, before, offset):
    row_count = normed.shape[0]
    lead_rows = before.shape[0]
    group_size = normed.shape[1] // len(WINDOWS)
    joined = jnp.concatenate([before, normed], axis=0).astype(jnp.float32)
    positions = offset + jnp.arange(row_count, dtype=jnp.int32)
    window_avg = []
    for group_idx, span in enumerate(WINDOWS):
        channels = joined[:, group_idx * group_size : (group_idx + 1) * group_size]
        first_row = lead_rows - span + 1
        running = channels[first_row : first_row + row_count]
        for shift_idx in range(1, span):
            running = running + channels[first_row + shift_idx : first_row + shift_idx + row_count]
        counts = jnp.minimum(positions + 1, span).astype(jnp.float32)
        window_avg.append(running / counts[:, None])
    return jnp.stack(window_avg, axis=1)


def fill_slots(normed, picks, expert_count, capacity):
    tok_count, top_count = picks.shape
    pair_count = tok_count * top_count
    flat_ids = picks.reshape(pair_count)
    matches = flat_ids[:, None] == jnp.arange(expert_count, dtype=jnp.int32)[None, :]
    pair_line = jnp.arange(pair_count, dtype=jnp.int32)
    lower_mask = (pair_line[:, None] > pair_line[None, :]).astype(jnp.bfloat16)
    seen_before = jnp.dot(
        lower_mask, matches.astype(jnp.bfloat16), preferred_element_type=jnp.float32
    )
    rank = jnp.sum(seen_before * matches.astype(jnp.float32), axis=1).astype(jnp.int32)
    slots = flat_ids * capacity + rank
    owner = pair_line // top_count
    slot_token = jnp.full((expert_count * capacity,), tok_count, jnp.int32).at[slots].set(owner)
    padded = jnp.concatenate([normed, jnp.zeros((1, normed.shape[1]), normed.dtype)], axis=0)
    return (padded[slot_token], slots.reshape(tok_count, top_count))


def blockwise_down(hidden, down_rows, pieces, contract):
    block_width = hidden.shape[-1] // pieces
    summed = None
    for part_idx in range(pieces):
        piece_out = jnp.einsum(
            contract,
            hidden[..., part_idx * block_width : (part_idx + 1) * block_width],
            down_rows[..., part_idx * block_width : (part_idx + 1) * block_width, :],
            preferred_element_type=jnp.float32,
        )
        summed = rounded(piece_out) if summed is None else summed + rounded(piece_out)
    return summed.astype(jnp.bfloat16)


def routed_by_slots(h_moe, expert_ids, route_w, expert_gate, expert_up, expert_down, shared_gate, shared_up, shared_down):
    tok_count, model_width = h_moe.shape
    top_count = expert_ids.shape[1]
    quarters = lax.axis_size("tp")
    my_quarter = lax.axis_index("tp")
    ep_count = lax.axis_size("ep")
    local_experts = expert_gate.shape[0]
    expert_count = ep_count * local_experts
    capacity = 3 * tok_count * top_count // (2 * expert_count)
    per_source = local_experts * capacity
    full_gate, full_up, full_down, full_sgate, full_sup, full_sdown = (
        lax.all_gather(expert_gate, "tp", axis=2, tiled=True),
        lax.all_gather(expert_up, "tp", axis=2, tiled=True),
        lax.all_gather(expert_down, "tp", axis=1, tiled=True),
        lax.all_gather(shared_gate, "tp", axis=1, tiled=True),
        lax.all_gather(shared_up, "tp", axis=1, tiled=True),
        lax.all_gather(shared_down, "tp", axis=0, tiled=True),
    )
    my_ids = lax.dynamic_slice_in_dim(expert_ids, my_quarter * tok_count, tok_count, 0)
    outgoing, my_slots = fill_slots(h_moe, my_ids, expert_count, capacity)
    landed = lax.all_to_all(
        outgoing.reshape(ep_count, per_source, model_width),
        "ep",
        split_axis=0,
        concat_axis=0,
        tiled=True,
    )
    routed_in = landed.reshape(ep_count, local_experts, capacity, model_width)
    gate_val = jnp.einsum(
        "necd,edf->necf", routed_in, full_gate, preferred_element_type=jnp.float32
    )
    up_val = jnp.einsum("necd,edf->necf", routed_in, full_up, preferred_element_type=jnp.float32)
    hidden = (jax.nn.silu(gate_val) * up_val).astype(jnp.bfloat16)
    expert_back = blockwise_down(hidden, full_down, quarters, "necf,efd->necd")
    expert_back = expert_back.reshape(ep_count, per_source, model_width)
    shared_gate_val = jnp.dot(h_moe, full_sgate, preferred_element_type=jnp.float32)
    shared_up_val = jnp.dot(h_moe, full_sup, preferred_element_type=jnp.float32)
    shared_hidden = (jax.nn.silu(shared_gate_val) * shared_up_val).astype(jnp.bfloat16)
    shared_back = blockwise_down(shared_hidden, full_sdown, quarters, "tf,fd->td")
    returned = lax.all_to_all(expert_back, "ep", split_axis=0, concat_axis=0, tiled=True)
    returned = returned.reshape(expert_count * capacity, model_width)
    combined = shared_back.astype(jnp.float32)
    for pick_idx in range(top_count):
        combined = combined + route_w[:, pick_idx : pick_idx + 1] * returned[
            my_slots[:, pick_idx]
        ].astype(jnp.float32)
    return combined.astype(jnp.bfloat16)


HALO = 16


def flat(dz, dy, dx):
    return dz * 4 + dy * 2 + dx


def build_tasks(gather_parts, reduce_parts, z_count, turns, units, block_us, cap_share):
    tasks = {}
    total = sum(part[1] for part in gather_parts)
    last = z_count - 1
    computed = {dz: ("unit", dz, len(units) - 1) for dz in range(z_count)}
    first_needs = {dz: [] for dz in range(z_count)}

    def local(name, cost, needs):
        tasks[name] = (needs, None, cost)

    for dz in range(z_count):
        for dx in range(2):
            if dz or dx:
                before = ("sz", 0, dz - 1, dx)
                link = "z" if dz else "x"
                needs = [before] if before in tasks else []
                tasks["sz", 0, dz, dx] = (needs, link, SHARE_US)
                first_needs[dz].append(("sz", 0, dz, dx))
            needs = [("sz", 0, dz, dx)] if dz or dx else []
            tasks["sy", 0, dz, dx] = (needs, "y", SHARE_US)
            first_needs[dz].append(("sy", 0, dz, dx))

    for p, (_, columns, order) in enumerate(gather_parts):
        scale = columns / total
        wide_x = order == "xzy"

        def message(name, link, rows, needs):
            tasks[name] = (needs, link, block_us * scale * rows)

        message(("fx", p), "x", 1.0, [])
        for dz in range(z_count):
            for dx in range(2):
                if dx and dz and not wide_x:
                    continue
                if dz:
                    before = ("fz", p, dz - 1, dx) if dz > 1 else ("fx", p)
                    message(("fz", p, dz, dx), "z", 1.0, [before] if dz > 1 or dx else [])
                    held = [("fz", p, dz, dx)]
                else:
                    held = [("fx", p)] if dx else []
                if dz or dx:
                    held.append(("sz", 0, dz, dx))
                local(("pack", p, dz, dx), 0.8 * scale + 0.1, held)
                first_needs[dz].append(("pack", p, dz, dx))
                if not dx or wide_x:
                    message(("gy", p, dz, dx), "y", cap_share, [("pack", p, dz, dx)])
                    first_needs[dz].append(("gy", p, dz, dx))
            if not wide_x:
                for dy in range(2):
                    if dz or dy:
                        source = ("gy", p, dz, 0) if dy else ("pack", p, dz, 0)
                        message(("gx", p, dz, dy), "x", cap_share, [source])
                        first_needs[dz].append(("gx", p, dz, dy))

    for p, (_, columns, order) in enumerate(reduce_parts):
        scale = columns / total
        wide_x = order == "xzy"

        def message(name, link, rows, needs):
            tasks[name] = (needs, link, block_us * scale * rows)

        for dz in range(z_count):
            for dx in range(2):
                if dx and dz and not wide_x:
                    continue
                ends = [computed[dz]]
                if not dx or wide_x:
                    sums = [computed[dz]] if wide_x else [("addx", p, dz, 1)]
                    message(("ry", p, dz, dx), "y", cap_share, sums)
                    ends.append(("ry", p, dz, dx))
                    if dz > 1:
                        ends.append(("rz", p, dz - 1, dx))
                    elif dz == 0:
                        ends.append(("rz", p, last, dx))
                if not wide_x and not dx and dz:
                    ends.append(("addx", p, dz, 0))
                if not dz and not dx:
                    ends.append(("rfx", p))
                local(("open", p, dz, dx), 1.0 * scale + 0.1, ends)
                if dz:
                    message(("rz", p, dz, dx), "z", 1.0, [("open", p, dz, dx)])
                elif dx:
                    message(("rfx", p), "x", 1.0, [("open", p, 0, 1)])
            if not wide_x:
                for dy in range(2):
                    if dz or dy:
                        message(("rx", p, dz, dy), "x", cap_share, [computed[dz]])
                        needs = [("rx", p, dz, dy), computed[dz]]
                        local(("addx", p, dz, dy), 0.4 * scale + 0.05, needs)
    before = None
    for dz in turns:
        for u, cost in enumerate(units):
            needs = first_needs[dz] if u == 0 else []
            local(("unit", dz, u), cost, ([before] if before else []) + needs)
            before = ("unit", dz, u)
    return tasks


def plan_steps(tasks, mixes, delay=2.5):
    after = {}
    for name, (needs, _, _) in tasks.items():
        for need in needs:
            after.setdefault(need, []).append(name)
    tail = {}

    def path(name):
        if name not in tail:
            _, link, cost = tasks[name]
            rest = max([path(q) for q in after.get(name, [])], default=0.0)
            tail[name] = cost + (delay if link else 0.0) + rest
        return tail[name]

    rank = sorted(tasks, key=lambda name: (-path(name) - EARLIER.get(name[0], 0), str(name)))
    clock, steps, done, started = 3.0, [], {}, set()
    free = {"x": 0.0, "y": 0.0, "z": 0.0}
    mixed = 0
    while len(started) < len(tasks):
        ready = [
            name
            for name in rank
            if name not in started
            and all(done.get(need, 1e9) <= clock for need in tasks[name][0])
        ]
        sends = [name for name in ready if tasks[name][1]]
        if sends:
            name = sends[0]
            _, link, cost = tasks[name]
            free[link] = max(clock, free[link]) + cost
            done[name] = free[link] + delay
            started.add(name)
            steps.append(name)
        elif ready:
            clock += tasks[ready[0]][2]
            done[ready[0]] = clock
            started.add(ready[0])
            steps.append(ready[0])
        else:
            arrival = min(t for t in done.values() if t > clock)
            gap = 0.1 if clock > MIX_ANYWHERE else 0.5
            if mixed < len(mixes) and (not mixed or clock > MIX_FROM) and arrival - clock > gap:
                steps.append(("mix", mixed))
                clock += mixes[mixed]
                mixed += 1
            else:
                clock = arrival
    steps.extend(("mix", i) for i in range(mixed, len(mixes)))
    return steps, clock


def norm_rows(source, gain_ref, target, row_count, target_row, first=0):
    rows = 32

    def one(i, _):
        start = pl.multiple_of(first + i * rows, rows)
        upcast = source[pl.ds(start, rows), :].astype(jnp.float32)
        scaled = upcast * lax.rsqrt(jnp.mean(upcast * upcast, axis=-1, keepdims=True) + RMS_EPS)
        goes = pl.multiple_of(start + target_row, 16)
        target[pl.ds(goes, rows), :] = (scaled * gain_ref[...]).astype(jnp.bfloat16)
        return 0

    lax.fori_loop(0, row_count // rows, one, 0, unroll=4)


def kernel(
    sizes,
    mix_in,
    mix_gain,
    pool_w,
    pool_scale,
    moe_in,
    moe_gain,
    ids_ref,
    score_ref,
    gate_in,
    up_in,
    down_in,
    sgate_in,
    sup_in,
    sdown_in,
    mix_out,
    moe_out,
    full_buf,
    packed_buf,
    packed_y,
    result_buf,
    result_land,
    sums_buf,
    sums_land,
    share_all,
    share_rows,
    rank_buf,
    before_buf,
    pick_buf,
    place_buf,
    slot_weight,
    gate_buf,
    up_buf,
    down_buf,
    sgate_buf,
    sup_buf,
    sdown_buf,
    hidden_buf,
    shared_hidden,
    moe_buf,
    mix_buf,
    pool_buf,
    normed_buf,
    diff_buf,
    local_sem,
    swap_send,
    swap_recv,
    block_send,
    block_recv,
    halo_send,
    halo_recv,
):
    z_count, tok, width, local, wide, swide, top, cap = sizes
    ep_count, tp_count = 2 * z_count, 4
    my_ep, my_tp = lax.axis_index("ep"), lax.axis_index("tp")
    my_z, my_y, my_x, my_core = my_ep // 2, my_ep % 2, my_tp // 2, my_tp % 2
    partner = (my_ep, my_x * 2 + (1 - my_core))
    device_count = ep_count * tp_count
    my_flat = my_ep * tp_count + my_tp
    blocks = [(dz, dy, dx) for dz in range(z_count) for dy in range(2) for dx in range(2)]
    bf16, f32 = jnp.bfloat16, jnp.float32

    def spot(dz, dy, dx):
        z = (my_z + dz) % z_count
        y = (my_y + dy) % 2
        x = (my_x + dx) % 2
        return (z * 2 + y, x * 2 + my_core)

    def at_flat(index):
        index = (index + device_count) % device_count
        return (index // tp_count, index % tp_count)

    loads = []

    def load(source, target):
        copy = pltpu.make_async_copy(source, target, local_sem.at[len(loads)])
        copy.start()
        loads.append(copy)
        return copy

    moe_load = load(moe_in, moe_buf)
    mix_load = load(mix_in, mix_buf)
    pairs = []
    for e in range(local):
        for source, target in ((gate_in, gate_buf), (up_in, up_buf)):
            pairs.append((source.at[e], target.at[e, 0], target.at[e, 1]))
    pairs.append((sgate_in, sgate_buf.at[:, pl.ds(0, swide)], sgate_buf.at[:, pl.ds(swide, swide)]))
    pairs.append((sup_in, sup_buf.at[:, pl.ds(0, swide)], sup_buf.at[:, pl.ds(swide, swide)]))
    pairs.append((sdown_in, sdown_buf.at[pl.ds(0, swide)], sdown_buf.at[pl.ds(swide, swide)]))
    for e in range(local):
        pairs.append((down_in.at[e], down_buf.at[e, 0], down_buf.at[e, 1]))
    weight_loads = [load(source, own) for source, own, _ in pairs]
    pool_load = load(pool_w, pool_buf)

    barrier = pltpu.get_barrier_semaphore()
    outer = at_flat(my_flat + 2 * my_core - 1)
    peers = [spot(1, 0, 0), spot(z_count - 1, 0, 0), spot(0, 1, 0), spot(0, 0, 1), partner]

    def greet(peer):
        pl.semaphore_signal(barrier, inc=1, device_id=peer, device_id_type=pl.DeviceIdType.MESH)

    for peer in peers:
        greet(peer)
    not_first, not_last = my_flat > 0, my_flat < device_count - 1
    has_outer = not_first & not_last

    @pl.when(has_outer)
    def _():
        greet(outer)

    scores = score_ref[...]
    ids_at = pl.ds(pl.multiple_of(my_tp * tok, tok), tok)
    share_all[0, 0:top, :] = ids_ref[:, ids_at].astype(f32)
    share_all[0, 4 : 4 + top, :] = scores / jnp.sum(scores, axis=0, keepdims=True) * ROUTED_SCALE
    line = lax.broadcasted_iota(jnp.int32, (8, tok), 0)
    expert = jnp.where(line < 4, my_ep, my_z * 2 + 1 - my_y) * local + line % 4
    expert = jnp.where(line % 4 < local, expert, -1).astype(f32)
    before_buf[...] = (
        lax.broadcasted_iota(jnp.int32, (tok, tok), 0)
        < lax.broadcasted_iota(jnp.int32, (tok, tok), 1)
    ).astype(f32).astype(bf16)

    moe_load.wait()
    norm_rows(moe_buf, moe_gain, full_buf.at[0], tok, 0)

    pl.semaphore_wait(barrier, len(peers) + has_outer.astype(jnp.int32))

    def remote(source, target, send, recv, device):
        return pltpu.make_async_remote_copy(
            src_ref=source,
            dst_ref=target,
            send_sem=send,
            recv_sem=recv,
            device_id=device,
            device_id_type=pl.DeviceIdType.MESH,
        )

    started = []

    def go(copy):
        copy.start()
        started.append(copy)
        return copy

    swaps = []

    def swap_weights():
        for i, (source, _, other) in enumerate(pairs):
            swaps.append(go(remote(source, other, swap_send.at[i], swap_recv.at[i], partner)))

    gather_parts, reduce_parts = column_parts(width, GATHER), column_parts(width, REDUCE)
    steps, tasks, numbers = plan(z_count, local, tok, width, cap)
    toward = {"z": (1, 0, 0), "y": (0, 1, 0), "x": (0, 0, 1)}
    every = pl.ds(0, local)

    def message(name):
        kind, p = name[0], name[1]
        part = (reduce_parts if kind in ("rx", "rfx", "ry", "rz") else gather_parts)[p]
        cols = pl.ds(part[0], part[1])

        def full(buf, dz, dx):
            return buf.at[dz * 2 + dx, :, cols]

        def packed(buf, dz, dy, dx):
            return buf.at[every, flat(dz, dy, dx), :, cols]

        if kind == "sz":
            _, _, dz, dx = name
            source = share_all.at[flat(dz - 1, 0, dx) if dz else 0]
            target, link = share_all.at[flat(dz, 0, dx)], "z" if dz else "x"
        elif kind == "sy":
            _, _, dz, dx = name
            source, target = share_all.at[flat(dz, 0, dx)], share_all.at[flat(dz, 1, dx)]
            link = "y"
        elif kind == "fx":
            source, target, link = full(full_buf, 0, 0), full(full_buf, 0, 1), "x"
        elif kind == "fz":
            _, _, dz, dx = name
            source, target, link = full(full_buf, dz - 1, dx), full(full_buf, dz, dx), "z"
        elif kind == "gy":
            _, _, dz, dx = name
            source = packed_y.at[every, dz * 2 + dx, :, cols]
            target, link = packed(packed_buf, dz, 1, dx), "y"
        elif kind == "gx":
            _, _, dz, dy = name
            source, target = packed(packed_buf, dz, dy, 0), packed(packed_buf, dz, dy, 1)
            link = "x"
        elif kind == "rx":
            _, _, dz, dy = name
            source, target = packed(result_buf, dz, dy, 1), packed(result_land, dz, dy, 1)
            link = "x"
        elif kind == "ry":
            _, _, dz, dx = name
            source, target = packed(result_buf, dz, 1, dx), packed(result_land, dz, 1, dx)
            link = "y"
        elif kind == "rz":
            _, _, dz, dx = name
            source, target, link = full(sums_buf, dz, dx), full(sums_land, dz, dx), "z"
        else:
            source, target, link = full(sums_buf, 0, 1), full(sums_land, 0, 1), "x"
        return remote(
            source,
            target,
            block_send.at[send_slot[name]],
            block_recv.at[numbers[name]],
            spot(*toward[link]),
        )

    send_slot, in_slot, used = {}, {}, {"x": 0, "y": 0, "z": 0}

    def start_message(name):
        link = tasks[name][1]
        slot = "xyz".index(link) * SEND_SLOTS + used[link] % SEND_SLOTS
        used[link] += 1
        if slot in in_slot:
            message(in_slot[slot]).wait_send()
        send_slot[name], in_slot[slot] = slot, name
        message(name).start()

    ranked = set()
    lines = list(range(local)) + list(range(4, 4 + local))

    def ensure_rank(b):
        if b in ranked:
            return
        ranked.add(b)
        rows = slice(flat(*b) * 8, flat(*b) * 8 + 8)
        chosen, weights = jnp.zeros((8, tok), f32), jnp.zeros((8, tok), f32)
        for pick in range(top):
            hit = share_all[flat(*b), pick : pick + 1, :] == expert
            chosen = jnp.where(hit, 1.0, chosen)
            weights = jnp.where(hit, share_all[flat(*b), 4 + pick : 5 + pick, :], weights)
        share_rows[rows, :] = weights
        count = jnp.dot(chosen.astype(bf16), before_buf[...], preferred_element_type=f32)
        rank_buf[rows, :] = jnp.where(chosen > 0.0, count, -1.0)

    def slot_rows(b, e):
        line = flat(*b) * 8 + e
        slots = lax.broadcasted_iota(jnp.int32, (cap, tok), 0).astype(f32)
        return rank_buf[line : line + 1, :] == slots, share_rows[line : line + 1, :]

    picked = set()

    def pack_unit(p, dz, dx):
        b, f = (dz, 0, dx), dz * 2 + dx
        if f not in picked:
            picked.add(f)
            ensure_rank(b)
            for i, e in enumerate(lines):
                hit, _ = slot_rows(b, e)
                pick_buf[f, i * cap : (i + 1) * cap, :] = jnp.where(hit, 1.0, 0.0).astype(bf16)
        cols = slice(gather_parts[p][0], gather_parts[p][0] + gather_parts[p][1])
        taken = lines if ("gy", p, dz, dx) in numbers else lines[:local]
        rows = jnp.dot(
            pick_buf[f, : len(taken) * cap, :], full_buf[f, :, cols], preferred_element_type=f32
        ).astype(bf16)
        for i in range(len(taken)):
            piece = rows[i * cap : (i + 1) * cap]
            if i < local:
                packed_buf[i, flat(*b), :, cols] = piece
            else:
                packed_y[i - local, f, :, cols] = piece

    placed = set()

    def open_unit(p, dz, dx):
        b, f = (dz, 0, dx), dz * 2 + dx
        slots = 2 * local * cap
        if f not in placed:
            placed.add(f)
            turned = rank_buf[flat(*b) * 8 : flat(*b) * 8 + 8, :].T
            lane = lax.broadcasted_iota(jnp.int32, (tok, slots), 1)
            rank = jnp.full((tok, slots), -1.0, f32)
            for i, e in enumerate(lines):
                rank = jnp.where(lane // cap == i, turned[:, e : e + 1], rank)
            hit = rank == (lane % cap).astype(f32)
            place_buf[f, :, :] = jnp.where(hit, 1.0, 0.0).astype(bf16)
        cols = slice(reduce_parts[p][0], reduce_parts[p][0] + reduce_parts[p][1])
        pieces = [result_buf[e, flat(*b), :, cols] for e in range(local)]
        if ("ry", p, dz, dx) in numbers:
            pieces += [result_land[e, flat(dz, 1, dx), :, cols] for e in range(local)]
        values = jnp.concatenate(pieces, axis=0)
        total = jnp.dot(
            place_buf[f, :, : len(pieces) * cap], values, preferred_element_type=f32
        )
        if dz == 0:
            total = total + jnp.dot(
                shared_hidden[dx * tok : (dx + 1) * tok, :],
                sdown_buf[:, cols],
                preferred_element_type=f32,
            )
        before = ("rz", p, dz - 1 if dz else z_count - 1, dx)
        if before in numbers and dz != 1:
            total = total + sums_land[before[2] * 2 + dx, :, cols].astype(f32)
        if dz == 0 and dx == 0:
            total = total + sums_land[1, :, cols].astype(f32)
            moe_out[:, cols] = total.astype(bf16)
        else:
            sums_buf[f, :, cols] = total.astype(bf16)

    def add_unit(p, dz, dy):
        cols = slice(reduce_parts[p][0], reduce_parts[p][0] + reduce_parts[p][1])
        for e in range(local):
            mine = result_buf[e, flat(dz, dy, 0), :, cols].astype(f32)
            other = result_land[e, flat(dz, dy, 1), :, cols].astype(f32)
            result_buf[e, flat(dz, dy, 0), :, cols] = (mine + other).astype(bf16)

    loaded = set()

    def have_weights(i, side):
        if (i, side) not in loaded:
            loaded.add((i, side))
            if side:
                swaps[i].wait_recv()
            else:
                weight_loads[i].wait()

    def hidden_unit(dz, unit):
        e, side = unit // 2, unit % 2
        if unit == 0:
            for at, b in enumerate(blocks[dz * 4 : dz * 4 + 4]):
                ensure_rank(b)
                for i in range(local):
                    hit, weights = slot_rows(b, i)
                    slot_weight[i, at * cap : (at + 1) * cap, :] = jnp.sum(
                        jnp.where(hit, weights, 0.0), axis=1, keepdims=True
                    )
        for i in (2 * e, 2 * e + 1):
            have_weights(i, side)
        rows = packed_buf[e, dz * 4 : dz * 4 + 4].reshape(4 * cap, width)
        gate_val = jnp.dot(rows, gate_buf[e, side], preferred_element_type=f32)
        up_val = jnp.dot(rows, up_buf[e, side], preferred_element_type=f32)
        hidden = jax.nn.silu(gate_val) * up_val * slot_weight[e]
        hidden_buf[e, :, side * wide : (side + 1) * wide] = hidden.astype(bf16)

    def shared_unit():
        for i in range(2 * local, 2 * local + 3):
            have_weights(i, 0)
            have_weights(i, 1)
        rows = full_buf[0:2].reshape(2 * tok, width)
        gate_val = jnp.dot(rows, sgate_buf[...], preferred_element_type=f32)
        up_val = jnp.dot(rows, sup_buf[...], preferred_element_type=f32)
        shared_hidden[...] = (jax.nn.silu(gate_val) * up_val).astype(bf16)

    def down_unit(dz, e):
        for side in range(2):
            have_weights(2 * local + 3 + e, side)
        count = width // 4
        for piece in range(4):
            cols = slice(piece * count, (piece + 1) * count)
            result = jnp.dot(
                hidden_buf[e],
                down_buf[e, :, :, cols].reshape(2 * wide, count),
                preferred_element_type=f32,
            )
            result_buf[e, dz * 4 : dz * 4 + 4, :, cols] = result.astype(bf16).reshape(4, cap, count)

    mix_rows = mix_in.shape[0]
    group = width // len(WINDOWS)
    halo_copy = remote(
        normed_buf.at[pl.ds(mix_rows, HALO)],
        normed_buf.at[pl.ds(0, HALO)],
        halo_send,
        halo_recv,
        at_flat(my_flat + 1),
    )

    def mix_unit(index):
        if index < 4:
            quarter = mix_rows // 4
            if index == 0:
                mix_load.wait()
            first = (index - 1) % 4 * quarter
            norm_rows(mix_buf, mix_gain, normed_buf, quarter, HALO, first)
            if index == 0:

                @pl.when(not_last)
                def _():
                    halo_copy.start()

            return
        g, side = (index - 4) // 2, (index - 4) % 2
        window = WINDOWS[g]
        cols = slice(g * group, (g + 1) * group)
        if index == 4:
            pool_load.wait()

            @pl.when(not_first)
            def _():
                halo_copy.wait_recv()

        rows, begin = 64, side * (mix_rows // 2)
        for start in range(begin, begin + mix_rows // 2, rows):
            joined = normed_buf[start : start + rows + HALO, cols].astype(f32)
            if start == 0:
                line = lax.broadcasted_iota(jnp.int32, joined.shape, 0)
                joined = jnp.where((line >= HALO) | (my_flat > 0), joined, 0.0)
            total, reach = joined, 1
            while reach < window:
                total = total + pltpu.roll(total, reach, 0)
                reach *= 2
            position = (
                my_flat * mix_rows + start + lax.broadcasted_iota(jnp.int32, (rows, group), 0)
            )
            taken = jnp.minimum(position + 1, window).astype(f32)
            pooled = total[HALO:] / taken
            diff_buf[start - begin : start - begin + rows, :] = (pooled - joined[HALO:]).astype(bf16)
        mixed = jnp.dot(diff_buf[...], pool_buf[g], preferred_element_type=f32)
        mix_out[begin : begin + mix_rows // 2, cols] = (mixed * pool_scale[:, cols]).astype(bf16)

    waited = set()
    for name in steps:
        if not swaps and name not in numbers:
            swap_weights()
        for need in tasks[name][0] if name in tasks else ():
            if need in numbers and need not in waited:
                waited.add(need)
                message(need).wait_recv()
        kind = name[0]
        if name in numbers:
            start_message(name)
        elif kind == "pack":
            pack_unit(*name[1:])
        elif kind == "open":
            open_unit(*name[1:])
        elif kind == "addx":
            add_unit(*name[1:])
        elif kind == "mix":
            mix_unit(name[1])
        elif name[2] < 2 * local:
            hidden_unit(name[1], name[2])
            if name[1] == 0 and name[2] == 2 * local - 1:
                shared_unit()
        else:
            down_unit(name[1], name[2] - 2 * local)
    for copy in started + [message(name) for name in in_slot.values()]:
        copy.wait_send()

    @pl.when(not_last)
    def _():
        halo_copy.wait_send()


def column_parts(width, pattern):
    lanes = width // 128
    parts, start, given = [], 0, 0
    for count, order in pattern:
        given += count
        stop = lanes * given // 16 * 128
        if stop > start:
            parts.append((start, stop - start, order))
        start = stop
    return parts


GATHER = ((5, "zyx"), (5, "zyx"), (3, "xzy"), (3, "xzy"))
REDUCE = ((4, "zyx"), (3, "zyx"), (3, "zyx"), (3, "xzy"), (3, "xzy"))
EARLIER = {"ry": 20, "fx": 5, "sz": 10, "sy": 20, "gy": -10, "rx": -2, "pack": 40, "rz": 5}
EARLIER |= {"rfx": -20, "open": 5, "fz": -5, "gx": 40, "unit": -5}
SHARE_US = 0.09
MIX_FROM, MIX_ANYWHERE = 30.0, 75.0
SEND_SLOTS = 12


@functools.lru_cache
def plan(z_count, local, tok, width, cap):
    turns = tuple(range(1, z_count)) + (0,)
    units = (0.5,) * (3 * local)
    tasks = build_tasks(
        column_parts(width, GATHER),
        column_parts(width, REDUCE),
        z_count,
        turns,
        units,
        tok * width * 2 / 46.6e3,
        local * cap / tok,
    )
    steps, _ = plan_steps(tasks, (0.5,) * 4 + (0.8,) * 2 * len(WINDOWS))
    names = [name for name in tasks if tasks[name][1]]
    return steps, tasks, {name: i for i, name in enumerate(names)}


def both_in_one_kernel(
    mix_input,
    mix_gain,
    pool_weight,
    pool_scale,
    moe_input,
    moe_gain,
    expert_ids,
    route_score,
    expert_gate,
    expert_up,
    expert_down,
    shared_gate,
    shared_up,
    shared_down,
):
    tok, width = moe_input.shape
    local, _, wide = expert_gate.shape
    swide = shared_gate.shape[1]
    z_count = lax.axis_size("ep") // 2
    top = expert_ids.shape[1]
    cap = 3 * tok * top // (4 * z_count * local)
    count = 4 * z_count
    mix_rows = mix_input.shape[0]
    group = width // len(WINDOWS)
    sizes = (z_count, tok, width, local, wide, swide, top, cap)
    pair_count = 3 * local + 3
    message_count = len(plan(z_count, local, tok, width, cap)[2])
    any_spec = pl.BlockSpec(memory_space=pl.ANY)
    vmem = pl.BlockSpec(memory_space=pltpu.VMEM)
    bf16, f32 = jnp.bfloat16, jnp.float32
    dma = pltpu.SemaphoreType.DMA
    flops = 2 * count * cap * local * width * 6 * wide + 2 * mix_rows * width * group
    return pl.pallas_call(
        functools.partial(kernel, sizes),
        out_shape=(pltpu.VMEM(mix_input.shape, bf16), pltpu.VMEM(moe_input.shape, bf16)),
        in_specs=[
            any_spec,
            vmem,
            any_spec,
            vmem,
            any_spec,
            vmem,
            vmem,
            vmem,
            any_spec,
            any_spec,
            any_spec,
            any_spec,
            any_spec,
            any_spec,
        ],
        out_specs=(vmem, vmem),
        scratch_shapes=[
            pltpu.VMEM((count // 2, tok, width), bf16),
            pltpu.VMEM((local, count, cap, width), bf16),
            pltpu.VMEM((local, count // 2, cap, width), bf16),
            pltpu.VMEM((local, count, cap, width), bf16),
            pltpu.VMEM((local, count, cap, width), bf16),
            pltpu.VMEM((count // 2, tok, width), bf16),
            pltpu.VMEM((count // 2, tok, width), bf16),
            pltpu.VMEM((count, 8, tok), f32),
            pltpu.VMEM((8 * count, tok), f32),
            pltpu.VMEM((8 * count, tok), f32),
            pltpu.VMEM((tok, tok), bf16),
            pltpu.VMEM((count // 2, 2 * local * cap, tok), bf16),
            pltpu.VMEM((count // 2, tok, 2 * local * cap), bf16),
            pltpu.VMEM((local, 4 * cap, 1), f32),
            pltpu.VMEM((local, 2, width, wide), bf16),
            pltpu.VMEM((local, 2, width, wide), bf16),
            pltpu.VMEM((local, 2, wide, width), bf16),
            pltpu.VMEM((width, 2 * swide), bf16),
            pltpu.VMEM((width, 2 * swide), bf16),
            pltpu.VMEM((2 * swide, width), bf16),
            pltpu.VMEM((local, 4 * cap, 2 * wide), bf16),
            pltpu.VMEM((2 * tok, 2 * swide), bf16),
            pltpu.VMEM(moe_input.shape, bf16),
            pltpu.VMEM(mix_input.shape, bf16),
            pltpu.VMEM(pool_weight.shape, bf16),
            pltpu.VMEM((mix_rows + HALO, width), bf16),
            pltpu.VMEM((mix_rows // 2, group), bf16),
            dma((pair_count + 3,)),
            dma((pair_count,)),
            dma((pair_count,)),
            dma((3 * SEND_SLOTS,)),
            dma((message_count,)),
            dma,
            dma,
        ],
        compiler_params=pltpu.CompilerParams(
            collective_id=0, has_side_effects=True, vmem_limit_bytes=59 * 1024 * 1024
        ),
        cost_estimate=pl.CostEstimate(flops=flops, bytes_accessed=24 << 20, transcendentals=0),
    )(
        mix_input,
        mix_gain.reshape(1, width),
        pool_weight,
        pool_scale.reshape(1, width),
        moe_input,
        moe_gain.reshape(1, width),
        expert_ids.T,
        route_score.T,
        expert_gate,
        expert_up,
        expert_down,
        shared_gate,
        shared_up,
        shared_down,
    )


def mixer(mix_input, mix_gain, pool_weight, pool_scale):
    normed = rms_norm(mix_input, mix_gain)
    row_count, width_all = normed.shape
    reach_rows = max(WINDOWS) - 1
    before = passed_along(normed[row_count - reach_rows :], ("ep", "tp"), 1)
    offset = lax.axis_index(("ep", "tp")) * row_count
    pooled = window_means(normed, before, offset)
    difference = (pooled - normed.astype(jnp.float32).reshape(row_count, len(WINDOWS), -1)).astype(
        jnp.bfloat16
    )
    mixed_out = jnp.einsum(
        "sgc,gcd->sgd", difference, pool_weight, preferred_element_type=jnp.float32
    )
    return (mixed_out.reshape(row_count, width_all) * pool_scale).astype(jnp.bfloat16)


def per_device(
    mix_input,
    mix_gain,
    pool_weight,
    pool_scale,
    moe_input,
    moe_gain,
    expert_ids,
    route_score,
    expert_gate,
    expert_up,
    expert_down,
    shared_gate,
    shared_up,
    shared_down,
):
    ep_count, tp_count = lax.axis_size("ep"), lax.axis_size("tp")
    few_experts = (
        ep_count * expert_gate.shape[0] <= 8 * expert_ids.shape[1]
        and ep_count % 2 == 0
        and 2 < ep_count <= 8
        and tp_count == 4
        and expert_gate.shape[0] <= 4
        and expert_ids.shape[1] <= 4
    )
    if few_experts:
        return both_in_one_kernel(
            mix_input,
            mix_gain,
            pool_weight,
            pool_scale,
            moe_input,
            moe_gain,
            expert_ids,
            route_score,
            expert_gate,
            expert_up,
            expert_down,
            shared_gate,
            shared_up,
            shared_down,
        )
    mix_output = mixer(mix_input, mix_gain, pool_weight, pool_scale)
    h_moe = rms_norm(moe_input, moe_gain)
    route_w = route_score / jnp.sum(route_score, axis=1, keepdims=True) * ROUTED_SCALE
    moe_output = routed_by_slots(
        h_moe,
        expert_ids,
        route_w,
        expert_gate,
        expert_up,
        expert_down,
        shared_gate,
        shared_up,
        shared_down,
    )
    return (mix_output, moe_output)


def solution(mesh):
    return jax.shard_map(
        per_device,
        mesh=mesh,
        in_specs=(
            P(("ep", "tp"), None),
            P(),
            P(),
            P(),
            P(("ep", "tp"), None),
            P(),
            P("ep", None),
            P(("ep", "tp"), None),
            P("ep", None, "tp"),
            P("ep", None, "tp"),
            P("ep", "tp", None),
            P(None, "tp"),
            P(None, "tp"),
            P("tp", None),
        ),
        out_specs=(P(("ep", "tp"), None), P(("ep", "tp"), None)),
        check_vma=False,
    )
```

```python
import functools

import jax
import jax.numpy as jnp
from jax import lax
from jax.experimental import pallas as pl
from jax.experimental.pallas import tpu as pltpu
from jax.sharding import PartitionSpec as P

WINDOWS = (2, 4, 8, 16)
RMS_EPS = 1e-06
ROUTED_SCALE = 2.5


def passed_along(value, axis, by):
    length = lax.axis_size(axis)
    pairs = [(i, i + by) for i in range(length) if 0 <= i + by < length]
    return lax.ppermute(value, axis, pairs)


def rms_norm(values, gain_row):
    upcast = values.astype(jnp.float32)
    scaled = upcast * lax.rsqrt(jnp.mean(upcast * upcast, axis=-1, keepdims=True) + RMS_EPS)
    return (scaled * gain_row).astype(jnp.bfloat16)


def rounded(values):
    return lax.optimization_barrier(values.astype(jnp.bfloat16)).astype(jnp.float32)


def window_means(normed, before, offset):
    row_count = normed.shape[0]
    lead_rows = before.shape[0]
    group_size = normed.shape[1] // len(WINDOWS)
    joined = jnp.concatenate([before, normed], axis=0).astype(jnp.float32)
    positions = offset + jnp.arange(row_count, dtype=jnp.int32)
    window_avg = []
    for group_idx, span in enumerate(WINDOWS):
        channels = joined[:, group_idx * group_size : (group_idx + 1) * group_size]
        first_row = lead_rows - span + 1
        running = channels[first_row : first_row + row_count]
        for shift_idx in range(1, span):
            running = running + channels[first_row + shift_idx : first_row + shift_idx + row_count]
        counts = jnp.minimum(positions + 1, span).astype(jnp.float32)
        window_avg.append(running / counts[:, None])
    return jnp.stack(window_avg, axis=1)


def fill_slots(normed, picks, expert_count, capacity):
    tok_count, top_count = picks.shape
    pair_count = tok_count * top_count
    flat_ids = picks.reshape(pair_count)
    matches = flat_ids[:, None] == jnp.arange(expert_count, dtype=jnp.int32)[None, :]
    pair_line = jnp.arange(pair_count, dtype=jnp.int32)
    lower_mask = (pair_line[:, None] > pair_line[None, :]).astype(jnp.bfloat16)
    seen_before = jnp.dot(
        lower_mask, matches.astype(jnp.bfloat16), preferred_element_type=jnp.float32
    )
    rank = jnp.sum(seen_before * matches.astype(jnp.float32), axis=1).astype(jnp.int32)
    slots = flat_ids * capacity + rank
    owner = pair_line // top_count
    slot_token = jnp.full((expert_count * capacity,), tok_count, jnp.int32).at[slots].set(owner)
    padded = jnp.concatenate([normed, jnp.zeros((1, normed.shape[1]), normed.dtype)], axis=0)
    return (padded[slot_token], slots.reshape(tok_count, top_count))


def blockwise_down(hidden, down_rows, pieces, contract):
    block_width = hidden.shape[-1] // pieces
    summed = None
    for part_idx in range(pieces):
        piece_out = jnp.einsum(
            contract,
            hidden[..., part_idx * block_width : (part_idx + 1) * block_width],
            down_rows[..., part_idx * block_width : (part_idx + 1) * block_width, :],
            preferred_element_type=jnp.float32,
        )
        summed = rounded(piece_out) if summed is None else summed + rounded(piece_out)
    return summed.astype(jnp.bfloat16)


def routed_by_slots(h_moe, expert_ids, route_w, expert_gate, expert_up, expert_down, shared_gate, shared_up, shared_down):
    tok_count, model_width = h_moe.shape
    top_count = expert_ids.shape[1]
    quarters = lax.axis_size("tp")
    my_quarter = lax.axis_index("tp")
    ep_count = lax.axis_size("ep")
    local_experts = expert_gate.shape[0]
    expert_count = ep_count * local_experts
    capacity = 3 * tok_count * top_count // (2 * expert_count)
    per_source = local_experts * capacity
    full_gate, full_up, full_down, full_sgate, full_sup, full_sdown = (
        lax.all_gather(expert_gate, "tp", axis=2, tiled=True),
        lax.all_gather(expert_up, "tp", axis=2, tiled=True),
        lax.all_gather(expert_down, "tp", axis=1, tiled=True),
        lax.all_gather(shared_gate, "tp", axis=1, tiled=True),
        lax.all_gather(shared_up, "tp", axis=1, tiled=True),
        lax.all_gather(shared_down, "tp", axis=0, tiled=True),
    )
    my_ids = lax.dynamic_slice_in_dim(expert_ids, my_quarter * tok_count, tok_count, 0)
    outgoing, my_slots = fill_slots(h_moe, my_ids, expert_count, capacity)
    landed = lax.all_to_all(
        outgoing.reshape(ep_count, per_source, model_width),
        "ep",
        split_axis=0,
        concat_axis=0,
        tiled=True,
    )
    routed_in = landed.reshape(ep_count, local_experts, capacity, model_width)
    gate_val = jnp.einsum(
        "necd,edf->necf", routed_in, full_gate, preferred_element_type=jnp.float32
    )
    up_val = jnp.einsum("necd,edf->necf", routed_in, full_up, preferred_element_type=jnp.float32)
    hidden = (jax.nn.silu(gate_val) * up_val).astype(jnp.bfloat16)
    expert_back = blockwise_down(hidden, full_down, quarters, "necf,efd->necd")
    expert_back = expert_back.reshape(ep_count, per_source, model_width)
    shared_gate_val = jnp.dot(h_moe, full_sgate, preferred_element_type=jnp.float32)
    shared_up_val = jnp.dot(h_moe, full_sup, preferred_element_type=jnp.float32)
    shared_hidden = (jax.nn.silu(shared_gate_val) * shared_up_val).astype(jnp.bfloat16)
    shared_back = blockwise_down(shared_hidden, full_sdown, quarters, "tf,fd->td")
    returned = lax.all_to_all(expert_back, "ep", split_axis=0, concat_axis=0, tiled=True)
    returned = returned.reshape(expert_count * capacity, model_width)
    combined = shared_back.astype(jnp.float32)
    for pick_idx in range(top_count):
        combined = combined + route_w[:, pick_idx : pick_idx + 1] * returned[
            my_slots[:, pick_idx]
        ].astype(jnp.float32)
    return combined.astype(jnp.bfloat16)


HALO = 16


def flat(dz, dy, dx):
    return dz * 4 + dy * 2 + dx


def build_tasks(gather_parts, reduce_parts, z_count, turns, units, block_us, cap_share):
    tasks = {}
    total = sum(part[1] for part in gather_parts)
    last = z_count - 1
    computed = {dz: ("unit", dz, len(units) - 1) for dz in range(z_count)}
    first_needs = {dz: [] for dz in range(z_count)}

    def local(name, cost, needs):
        tasks[name] = (needs, None, cost)

    for dz in range(z_count):
        for dx in range(2):
            if dz or dx:
                before = ("sz", 0, dz - 1, dx)
                link = "z" if dz else "x"
                needs = [before] if before in tasks else []
                tasks["sz", 0, dz, dx] = (needs, link, SHARE_US)
                first_needs[dz].append(("sz", 0, dz, dx))
            needs = [("sz", 0, dz, dx)] if dz or dx else []
            tasks["sy", 0, dz, dx] = (needs, "y", SHARE_US)
            first_needs[dz].append(("sy", 0, dz, dx))

    for p, (_, columns, order) in enumerate(gather_parts):
        scale = columns / total
        wide_x = order == "xzy"

        def message(name, link, rows, needs):
            tasks[name] = (needs, link, block_us * scale * rows)

        message(("fx", p), "x", 1.0, [])
        for dz in range(z_count):
            for dx in range(2):
                if dx and dz and not wide_x:
                    continue
                if dz:
                    before = ("fz", p, dz - 1, dx) if dz > 1 else ("fx", p)
                    message(("fz", p, dz, dx), "z", 1.0, [before] if dz > 1 or dx else [])
                    held = [("fz", p, dz, dx)]
                else:
                    held = [("fx", p)] if dx else []
                if dz or dx:
                    held.append(("sz", 0, dz, dx))
                local(("pack", p, dz, dx), 0.8 * scale + 0.1, held)
                first_needs[dz].append(("pack", p, dz, dx))
                if not dx or wide_x:
                    message(("gy", p, dz, dx), "y", cap_share, [("pack", p, dz, dx)])
                    first_needs[dz].append(("gy", p, dz, dx))
            if not wide_x:
                for dy in range(2):
                    if dz or dy:
                        source = ("gy", p, dz, 0) if dy else ("pack", p, dz, 0)
                        message(("gx", p, dz, dy), "x", cap_share, [source])
                        first_needs[dz].append(("gx", p, dz, dy))

    for p, (_, columns, order) in enumerate(reduce_parts):
        scale = columns / total
        wide_x = order == "xzy"

        def message(name, link, rows, needs):
            tasks[name] = (needs, link, block_us * scale * rows)

        for dz in range(z_count):
            for dx in range(2):
                if dx and dz and not wide_x:
                    continue
                ends = [computed[dz]]
                if not dx or wide_x:
                    sums = [computed[dz]] if wide_x else [("addx", p, dz, 1)]
                    message(("ry", p, dz, dx), "y", cap_share, sums)
                    ends.append(("ry", p, dz, dx))
                    if dz > 1:
                        ends.append(("rz", p, dz - 1, dx))
                    elif dz == 0:
                        ends.append(("rz", p, last, dx))
                if not wide_x and not dx and dz:
                    ends.append(("addx", p, dz, 0))
                if not dz and not dx:
                    ends.append(("rfx", p))
                local(("open", p, dz, dx), 1.0 * scale + 0.1, ends)
                if dz:
                    message(("rz", p, dz, dx), "z", 1.0, [("open", p, dz, dx)])
                elif dx:
                    message(("rfx", p), "x", 1.0, [("open", p, 0, 1)])
            if not wide_x:
                for dy in range(2):
                    if dz or dy:
                        message(("rx", p, dz, dy), "x", cap_share, [computed[dz]])
                        needs = [("rx", p, dz, dy), computed[dz]]
                        local(("addx", p, dz, dy), 0.4 * scale + 0.05, needs)
    before = None
    for dz in turns:
        for u, cost in enumerate(units):
            needs = first_needs[dz] if u == 0 else []
            local(("unit", dz, u), cost, ([before] if before else []) + needs)
            before = ("unit", dz, u)
    return tasks


def plan_steps(tasks, mixes, delay=2.5):
    after = {}
    for name, (needs, _, _) in tasks.items():
        for need in needs:
            after.setdefault(need, []).append(name)
    tail = {}

    def path(name):
        if name not in tail:
            _, link, cost = tasks[name]
            rest = max([path(q) for q in after.get(name, [])], default=0.0)
            tail[name] = cost + (delay if link else 0.0) + rest
        return tail[name]

    rank = sorted(tasks, key=lambda name: (-path(name) - EARLIER.get(name[0], 0), str(name)))
    clock, steps, done, started = 3.0, [], {}, set()
    free = {"x": 0.0, "y": 0.0, "z": 0.0}
    mixed = 0
    while len(started) < len(tasks):
        ready = [
            name
            for name in rank
            if name not in started
            and all(done.get(need, 1e9) <= clock for need in tasks[name][0])
        ]
        sends = [name for name in ready if tasks[name][1]]
        if sends:
            name = sends[0]
            _, link, cost = tasks[name]
            free[link] = max(clock, free[link]) + cost
            done[name] = free[link] + delay
            started.add(name)
            steps.append(name)
        elif ready:
            clock += tasks[ready[0]][2]
            done[ready[0]] = clock
            started.add(ready[0])
            steps.append(ready[0])
        else:
            arrival = min(t for t in done.values() if t > clock)
            gap = 0.1 if clock > MIX_ANYWHERE else 0.5
            if mixed < len(mixes) and (not mixed or clock > MIX_FROM) and arrival - clock > gap:
                steps.append(("mix", mixed))
                clock += mixes[mixed]
                mixed += 1
            else:
                clock = arrival
    steps.extend(("mix", i) for i in range(mixed, len(mixes)))
    return steps, clock


def norm_rows(source, gain_ref, target, row_count, target_row, first=0):
    rows = 32

    def one(i, _):
        start = pl.multiple_of(first + i * rows, rows)
        upcast = source[pl.ds(start, rows), :].astype(jnp.float32)
        scaled = upcast * lax.rsqrt(jnp.mean(upcast * upcast, axis=-1, keepdims=True) + RMS_EPS)
        goes = pl.multiple_of(start + target_row, 16)
        target[pl.ds(goes, rows), :] = (scaled * gain_ref[...]).astype(jnp.bfloat16)
        return 0

    lax.fori_loop(0, row_count // rows, one, 0, unroll=4)


def kernel(
    sizes,
    mix_in,
    mix_gain,
    pool_w,
    pool_scale,
    moe_in,
    moe_gain,
    ids_ref,
    score_ref,
    gate_in,
    up_in,
    down_in,
    sgate_in,
    sup_in,
    sdown_in,
    mix_out,
    moe_out,
    full_buf,
    packed_buf,
    packed_y,
    result_buf,
    result_land,
    sums_buf,
    sums_land,
    share_all,
    share_rows,
    rank_buf,
    before_buf,
    pick_buf,
    place_buf,
    slot_weight,
    gate_buf,
    up_buf,
    down_buf,
    sgate_buf,
    sup_buf,
    sdown_buf,
    hidden_buf,
    shared_hidden,
    moe_buf,
    mix_buf,
    pool_buf,
    normed_buf,
    diff_buf,
    local_sem,
    swap_send,
    swap_recv,
    block_send,
    block_recv,
    halo_send,
    halo_recv,
):
    z_count, tok, width, local, wide, swide, top, cap = sizes
    ep_count, tp_count = 2 * z_count, 4
    my_ep, my_tp = lax.axis_index("ep"), lax.axis_index("tp")
    my_z, my_y, my_x, my_core = my_ep // 2, my_ep % 2, my_tp // 2, my_tp % 2
    partner = (my_ep, my_x * 2 + (1 - my_core))
    device_count = ep_count * tp_count
    my_flat = my_ep * tp_count + my_tp
    blocks = [(dz, dy, dx) for dz in range(z_count) for dy in range(2) for dx in range(2)]
    bf16, f32 = jnp.bfloat16, jnp.float32

    def spot(dz, dy, dx):
        z = (my_z + dz) % z_count
        y = (my_y + dy) % 2
        x = (my_x + dx) % 2
        return (z * 2 + y, x * 2 + my_core)

    def at_flat(index):
        index = (index + device_count) % device_count
        return (index // tp_count, index % tp_count)

    barrier = pltpu.get_barrier_semaphore()
    outer = at_flat(my_flat + 2 * my_core - 1)
    peers = [spot(1, 0, 0), spot(z_count - 1, 0, 0), spot(0, 1, 0), spot(0, 0, 1), partner]

    def greet(peer):
        pl.semaphore_signal(barrier, inc=1, device_id=peer, device_id_type=pl.DeviceIdType.MESH)

    for peer in peers:
        greet(peer)
    not_first, not_last = my_flat > 0, my_flat < device_count - 1
    has_outer = not_first & not_last

    @pl.when(has_outer)
    def _():
        greet(outer)

    loads = []

    def load(source, target):
        copy = pltpu.make_async_copy(source, target, local_sem.at[len(loads)])
        copy.start()
        loads.append(copy)
        return copy

    moe_load = load(moe_in, moe_buf)
    mix_load = load(mix_in, mix_buf)
    pairs = []
    for e in range(local):
        for source, target in ((gate_in, gate_buf), (up_in, up_buf)):
            pairs.append((source.at[e], target.at[e, 0], target.at[e, 1]))
    pairs.append((sgate_in, sgate_buf.at[:, pl.ds(0, swide)], sgate_buf.at[:, pl.ds(swide, swide)]))
    pairs.append((sup_in, sup_buf.at[:, pl.ds(0, swide)], sup_buf.at[:, pl.ds(swide, swide)]))
    pairs.append((sdown_in, sdown_buf.at[pl.ds(0, swide)], sdown_buf.at[pl.ds(swide, swide)]))
    for e in range(local):
        pairs.append((down_in.at[e], down_buf.at[e, 0], down_buf.at[e, 1]))
    weight_loads = [load(source, own) for source, own, _ in pairs]
    pool_load = load(pool_w, pool_buf)

    scores = score_ref[...]
    ids_at = pl.ds(pl.multiple_of(my_tp * tok, tok), tok)
    share_all[0, 0:top, :] = ids_ref[:, ids_at].astype(f32)
    share_all[0, 4 : 4 + top, :] = scores / jnp.sum(scores, axis=0, keepdims=True) * ROUTED_SCALE
    line = lax.broadcasted_iota(jnp.int32, (8, tok), 0)
    expert = jnp.where(line < 4, my_ep, my_z * 2 + 1 - my_y) * local + line % 4
    expert = jnp.where(line % 4 < local, expert, -1).astype(f32)
    moe_load.wait()
    norm_rows(moe_buf, moe_gain, full_buf.at[0], tok, 0)

    pl.semaphore_wait(barrier, len(peers) + has_outer.astype(jnp.int32))

    def remote(source, target, send, recv, device):
        return pltpu.make_async_remote_copy(
            src_ref=source,
            dst_ref=target,
            send_sem=send,
            recv_sem=recv,
            device_id=device,
            device_id_type=pl.DeviceIdType.MESH,
        )

    started = []

    def go(copy):
        copy.start()
        started.append(copy)
        return copy

    swaps = []

    def swap_weights():
        for i, (source, _, other) in enumerate(pairs):
            swaps.append(go(remote(source, other, swap_send.at[i], swap_recv.at[i], partner)))

    gather_parts, reduce_parts = column_parts(width, GATHER), column_parts(width, REDUCE)
    steps, tasks, numbers = plan(z_count, local, tok, width, cap)
    toward = {"z": (1, 0, 0), "y": (0, 1, 0), "x": (0, 0, 1)}
    every = pl.ds(0, local)

    def message(name):
        kind, p = name[0], name[1]
        part = (reduce_parts if kind in ("rx", "rfx", "ry", "rz") else gather_parts)[p]
        cols = pl.ds(part[0], part[1])

        def full(buf, dz, dx):
            return buf.at[dz * 2 + dx, :, cols]

        def packed(buf, dz, dy, dx):
            return buf.at[every, flat(dz, dy, dx), :, cols]

        if kind == "sz":
            _, _, dz, dx = name
            source = share_all.at[flat(dz - 1, 0, dx) if dz else 0]
            target, link = share_all.at[flat(dz, 0, dx)], "z" if dz else "x"
        elif kind == "sy":
            _, _, dz, dx = name
            source, target = share_all.at[flat(dz, 0, dx)], share_all.at[flat(dz, 1, dx)]
            link = "y"
        elif kind == "fx":
            source, target, link = full(full_buf, 0, 0), full(full_buf, 0, 1), "x"
        elif kind == "fz":
            _, _, dz, dx = name
            source, target, link = full(full_buf, dz - 1, dx), full(full_buf, dz, dx), "z"
        elif kind == "gy":
            _, _, dz, dx = name
            source = packed_y.at[every, dz * 2 + dx, :, cols]
            target, link = packed(packed_buf, dz, 1, dx), "y"
        elif kind == "gx":
            _, _, dz, dy = name
            source, target = packed(packed_buf, dz, dy, 0), packed(packed_buf, dz, dy, 1)
            link = "x"
        elif kind == "rx":
            _, _, dz, dy = name
            source, target = packed(result_buf, dz, dy, 1), packed(result_land, dz, dy, 1)
            link = "x"
        elif kind == "ry":
            _, _, dz, dx = name
            source, target = packed(result_buf, dz, 1, dx), packed(result_land, dz, 1, dx)
            link = "y"
        elif kind == "rz":
            _, _, dz, dx = name
            source, target, link = full(sums_buf, dz, dx), full(sums_land, dz, dx), "z"
        else:
            source, target, link = full(sums_buf, 0, 1), full(sums_land, 0, 1), "x"
        return remote(
            source,
            target,
            block_send.at[send_slot[name]],
            block_recv.at[numbers[name]],
            spot(*toward[link]),
        )

    send_slot, in_slot, used = {}, {}, {"x": 0, "y": 0, "z": 0}

    def start_message(name):
        link = tasks[name][1]
        slot = "xyz".index(link) * SEND_SLOTS + used[link] % SEND_SLOTS
        used[link] += 1
        if slot in in_slot:
            message(in_slot[slot]).wait_send()
        send_slot[name], in_slot[slot] = slot, name
        message(name).start()

    ranked = set()
    lines = list(range(local)) + list(range(4, 4 + local))

    def ensure_rank(b):
        if b in ranked:
            return
        ranked.add(b)
        rows = slice(flat(*b) * 8, flat(*b) * 8 + 8)
        chosen, weights = jnp.zeros((8, tok), f32), jnp.zeros((8, tok), f32)
        for pick in range(top):
            hit = share_all[flat(*b), pick : pick + 1, :] == expert
            chosen = jnp.where(hit, 1.0, chosen)
            weights = jnp.where(hit, share_all[flat(*b), 4 + pick : 5 + pick, :], weights)
        share_rows[rows, :] = weights
        count = jnp.dot(chosen.astype(bf16), before_buf[...], preferred_element_type=f32)
        rank_buf[rows, :] = jnp.where(chosen > 0.0, count, -1.0)

    def slot_rows(b, e):
        line = flat(*b) * 8 + e
        slots = lax.broadcasted_iota(jnp.int32, (cap, tok), 0).astype(f32)
        return rank_buf[line : line + 1, :] == slots, share_rows[line : line + 1, :]

    picked = set()

    def pack_unit(p, dz, dx):
        b, f = (dz, 0, dx), dz * 2 + dx
        if f not in picked:
            picked.add(f)
            ensure_rank(b)
            for i, e in enumerate(lines):
                hit, _ = slot_rows(b, e)
                pick_buf[f, i * cap : (i + 1) * cap, :] = jnp.where(hit, 1.0, 0.0).astype(bf16)
        cols = slice(gather_parts[p][0], gather_parts[p][0] + gather_parts[p][1])
        taken = lines if ("gy", p, dz, dx) in numbers else lines[:local]
        rows = jnp.dot(
            pick_buf[f, : len(taken) * cap, :], full_buf[f, :, cols], preferred_element_type=f32
        ).astype(bf16)
        for i in range(len(taken)):
            piece = rows[i * cap : (i + 1) * cap]
            if i < local:
                packed_buf[i, flat(*b), :, cols] = piece
            else:
                packed_y[i - local, f, :, cols] = piece

    placed = set()

    def open_unit(p, dz, dx):
        b, f = (dz, 0, dx), dz * 2 + dx
        slots = 2 * local * cap
        if f not in placed:
            placed.add(f)
            turned = rank_buf[flat(*b) * 8 : flat(*b) * 8 + 8, :].T
            lane = lax.broadcasted_iota(jnp.int32, (tok, slots), 1)
            rank = jnp.full((tok, slots), -1.0, f32)
            for i, e in enumerate(lines):
                rank = jnp.where(lane // cap == i, turned[:, e : e + 1], rank)
            hit = rank == (lane % cap).astype(f32)
            place_buf[f, :, :] = jnp.where(hit, 1.0, 0.0).astype(bf16)
        cols = slice(reduce_parts[p][0], reduce_parts[p][0] + reduce_parts[p][1])
        pieces = [result_buf[e, flat(*b), :, cols] for e in range(local)]
        if ("ry", p, dz, dx) in numbers:
            pieces += [result_land[e, flat(dz, 1, dx), :, cols] for e in range(local)]
        values = jnp.concatenate(pieces, axis=0)
        total = jnp.dot(
            place_buf[f, :, : len(pieces) * cap], values, preferred_element_type=f32
        )
        if dz == 0:
            total = total + jnp.dot(
                shared_hidden[dx * tok : (dx + 1) * tok, :],
                sdown_buf[:, cols],
                preferred_element_type=f32,
            )
        before = ("rz", p, dz - 1 if dz else z_count - 1, dx)
        if before in numbers and dz != 1:
            total = total + sums_land[before[2] * 2 + dx, :, cols].astype(f32)
        if dz == 0 and dx == 0:
            total = total + sums_land[1, :, cols].astype(f32)
            moe_out[:, cols] = total.astype(bf16)
        else:
            sums_buf[f, :, cols] = total.astype(bf16)

    def add_unit(p, dz, dy):
        cols = slice(reduce_parts[p][0], reduce_parts[p][0] + reduce_parts[p][1])
        for e in range(local):
            mine = result_buf[e, flat(dz, dy, 0), :, cols].astype(f32)
            other = result_land[e, flat(dz, dy, 1), :, cols].astype(f32)
            result_buf[e, flat(dz, dy, 0), :, cols] = (mine + other).astype(bf16)

    loaded = set()

    def have_weights(i, side):
        if (i, side) not in loaded:
            loaded.add((i, side))
            if side:
                swaps[i].wait_recv()
            else:
                weight_loads[i].wait()

    def hidden_unit(dz, unit):
        e, side = unit // 2, unit % 2
        if unit == 0:
            for at, b in enumerate(blocks[dz * 4 : dz * 4 + 4]):
                ensure_rank(b)
                for i in range(local):
                    hit, weights = slot_rows(b, i)
                    slot_weight[i, at * cap : (at + 1) * cap, :] = jnp.sum(
                        jnp.where(hit, weights, 0.0), axis=1, keepdims=True
                    )
        for i in (2 * e, 2 * e + 1):
            have_weights(i, side)
        rows = packed_buf[e, dz * 4 : dz * 4 + 4].reshape(4 * cap, width)
        gate_val = jnp.dot(rows, gate_buf[e, side], preferred_element_type=f32)
        up_val = jnp.dot(rows, up_buf[e, side], preferred_element_type=f32)
        hidden = jax.nn.silu(gate_val) * up_val * slot_weight[e]
        hidden_buf[e, :, side * wide : (side + 1) * wide] = hidden.astype(bf16)

    def shared_unit():
        for i in range(2 * local, 2 * local + 3):
            have_weights(i, 0)
            have_weights(i, 1)
        rows = full_buf[0:2].reshape(2 * tok, width)
        gate_val = jnp.dot(rows, sgate_buf[...], preferred_element_type=f32)
        up_val = jnp.dot(rows, sup_buf[...], preferred_element_type=f32)
        shared_hidden[...] = (jax.nn.silu(gate_val) * up_val).astype(bf16)

    def down_unit(dz, e):
        for side in range(2):
            have_weights(2 * local + 3 + e, side)
        count = width // 4
        for piece in range(4):
            cols = slice(piece * count, (piece + 1) * count)
            result = jnp.dot(
                hidden_buf[e],
                down_buf[e, :, :, cols].reshape(2 * wide, count),
                preferred_element_type=f32,
            )
            result_buf[e, dz * 4 : dz * 4 + 4, :, cols] = result.astype(bf16).reshape(4, cap, count)

    mix_rows = mix_in.shape[0]
    group = width // len(WINDOWS)
    halo_copy = remote(
        normed_buf.at[pl.ds(mix_rows, HALO)],
        normed_buf.at[pl.ds(0, HALO)],
        halo_send,
        halo_recv,
        at_flat(my_flat + 1),
    )

    def mix_unit(index):
        if index < 4:
            quarter = mix_rows // 4
            if index == 0:
                mix_load.wait()
            first = (index - 1) % 4 * quarter
            norm_rows(mix_buf, mix_gain, normed_buf, quarter, HALO, first)
            if index == 0:

                @pl.when(not_last)
                def _():
                    halo_copy.start()

            return
        g, side = (index - 4) // 2, (index - 4) % 2
        window = WINDOWS[g]
        cols = slice(g * group, (g + 1) * group)
        if index == 4:
            pool_load.wait()

            @pl.when(not_first)
            def _():
                halo_copy.wait_recv()

        rows, begin = 64, side * (mix_rows // 2)
        for start in range(begin, begin + mix_rows // 2, rows):
            joined = normed_buf[start : start + rows + HALO, cols].astype(f32)
            if start == 0:
                line = lax.broadcasted_iota(jnp.int32, joined.shape, 0)
                joined = jnp.where((line >= HALO) | (my_flat > 0), joined, 0.0)
            total, reach = joined, 1
            while reach < window:
                total = total + pltpu.roll(total, reach, 0)
                reach *= 2
            position = (
                my_flat * mix_rows + start + lax.broadcasted_iota(jnp.int32, (rows, group), 0)
            )
            taken = jnp.minimum(position + 1, window).astype(f32)
            pooled = total[HALO:] / taken
            diff_buf[start - begin : start - begin + rows, :] = (pooled - joined[HALO:]).astype(bf16)
        mixed = jnp.dot(diff_buf[...], pool_buf[g], preferred_element_type=f32)
        mix_out[begin : begin + mix_rows // 2, cols] = (mixed * pool_scale[:, cols]).astype(bf16)

    waited = set()
    for name in steps:
        if not swaps and name not in numbers:
            swap_weights()
            before_buf[...] = (
                lax.broadcasted_iota(jnp.int32, (tok, tok), 0)
                < lax.broadcasted_iota(jnp.int32, (tok, tok), 1)
            ).astype(f32).astype(bf16)
        for need in tasks[name][0] if name in tasks else ():
            if need in numbers and need not in waited:
                waited.add(need)
                message(need).wait_recv()
        kind = name[0]
        if name in numbers:
            start_message(name)
        elif kind == "pack":
            pack_unit(*name[1:])
        elif kind == "open":
            open_unit(*name[1:])
        elif kind == "addx":
            add_unit(*name[1:])
        elif kind == "mix":
            mix_unit(name[1])
        elif name[2] < 2 * local:
            hidden_unit(name[1], name[2])
            if name[1] == 0 and name[2] == 2 * local - 1:
                shared_unit()
        else:
            down_unit(name[1], name[2] - 2 * local)
    for copy in started + [message(name) for name in in_slot.values()]:
        copy.wait_send()

    @pl.when(not_last)
    def _():
        halo_copy.wait_send()


def column_parts(width, pattern):
    lanes = width // 128
    parts, start, given = [], 0, 0
    for count, order in pattern:
        given += count
        stop = lanes * given // 16 * 128
        if stop > start:
            parts.append((start, stop - start, order))
        start = stop
    return parts


GATHER = ((5, "zyx"), (5, "zyx"), (3, "xzy"), (3, "xzy"))
REDUCE = ((4, "zyx"), (3, "zyx"), (3, "zyx"), (3, "xzy"), (3, "xzy"))
EARLIER = {"ry": 20, "fx": 5, "sz": 10, "sy": 20, "gy": -10, "rx": -2, "pack": 40, "rz": 5}
EARLIER |= {"rfx": -20, "open": 5, "fz": -5, "gx": 40, "unit": -5}
SHARE_US = 0.09
MIX_FROM, MIX_ANYWHERE = 30.0, 75.0
SEND_SLOTS = 12


@functools.lru_cache
def plan(z_count, local, tok, width, cap):
    turns = tuple(range(1, z_count)) + (0,)
    units = (0.5,) * (3 * local)
    tasks = build_tasks(
        column_parts(width, GATHER),
        column_parts(width, REDUCE),
        z_count,
        turns,
        units,
        tok * width * 2 / 46.6e3,
        local * cap / tok,
    )
    steps, _ = plan_steps(tasks, (0.5,) * 4 + (0.8,) * 2 * len(WINDOWS))
    names = [name for name in tasks if tasks[name][1]]
    return steps, tasks, {name: i for i, name in enumerate(names)}


def both_in_one_kernel(
    mix_input,
    mix_gain,
    pool_weight,
    pool_scale,
    moe_input,
    moe_gain,
    expert_ids,
    route_score,
    expert_gate,
    expert_up,
    expert_down,
    shared_gate,
    shared_up,
    shared_down,
):
    tok, width = moe_input.shape
    local, _, wide = expert_gate.shape
    swide = shared_gate.shape[1]
    z_count = lax.axis_size("ep") // 2
    top = expert_ids.shape[1]
    cap = 3 * tok * top // (4 * z_count * local)
    count = 4 * z_count
    mix_rows = mix_input.shape[0]
    group = width // len(WINDOWS)
    sizes = (z_count, tok, width, local, wide, swide, top, cap)
    pair_count = 3 * local + 3
    message_count = len(plan(z_count, local, tok, width, cap)[2])
    any_spec = pl.BlockSpec(memory_space=pl.ANY)
    vmem = pl.BlockSpec(memory_space=pltpu.VMEM)
    bf16, f32 = jnp.bfloat16, jnp.float32
    dma = pltpu.SemaphoreType.DMA
    flops = 2 * count * cap * local * width * 6 * wide + 2 * mix_rows * width * group
    return pl.pallas_call(
        functools.partial(kernel, sizes),
        out_shape=(pltpu.VMEM(mix_input.shape, bf16), pltpu.VMEM(moe_input.shape, bf16)),
        in_specs=[
            any_spec,
            vmem,
            any_spec,
            vmem,
            any_spec,
            vmem,
            vmem,
            vmem,
            any_spec,
            any_spec,
            any_spec,
            any_spec,
            any_spec,
            any_spec,
        ],
        out_specs=(vmem, vmem),
        scratch_shapes=[
            pltpu.VMEM((count // 2, tok, width), bf16),
            pltpu.VMEM((local, count, cap, width), bf16),
            pltpu.VMEM((local, count // 2, cap, width), bf16),
            pltpu.VMEM((local, count, cap, width), bf16),
            pltpu.VMEM((local, count, cap, width), bf16),
            pltpu.VMEM((count // 2, tok, width), bf16),
            pltpu.VMEM((count // 2, tok, width), bf16),
            pltpu.VMEM((count, 8, tok), f32),
            pltpu.VMEM((8 * count, tok), f32),
            pltpu.VMEM((8 * count, tok), f32),
            pltpu.VMEM((tok, tok), bf16),
            pltpu.VMEM((count // 2, 2 * local * cap, tok), bf16),
            pltpu.VMEM((count // 2, tok, 2 * local * cap), bf16),
            pltpu.VMEM((local, 4 * cap, 1), f32),
            pltpu.VMEM((local, 2, width, wide), bf16),
            pltpu.VMEM((local, 2, width, wide), bf16),
            pltpu.VMEM((local, 2, wide, width), bf16),
            pltpu.VMEM((width, 2 * swide), bf16),
            pltpu.VMEM((width, 2 * swide), bf16),
            pltpu.VMEM((2 * swide, width), bf16),
            pltpu.VMEM((local, 4 * cap, 2 * wide), bf16),
            pltpu.VMEM((2 * tok, 2 * swide), bf16),
            pltpu.VMEM(moe_input.shape, bf16),
            pltpu.VMEM(mix_input.shape, bf16),
            pltpu.VMEM(pool_weight.shape, bf16),
            pltpu.VMEM((mix_rows + HALO, width), bf16),
            pltpu.VMEM((mix_rows // 2, group), bf16),
            dma((pair_count + 3,)),
            dma((pair_count,)),
            dma((pair_count,)),
            dma((3 * SEND_SLOTS,)),
            dma((message_count,)),
            dma,
            dma,
        ],
        compiler_params=pltpu.CompilerParams(
            collective_id=0, has_side_effects=True, vmem_limit_bytes=59 * 1024 * 1024
        ),
        cost_estimate=pl.CostEstimate(flops=flops, bytes_accessed=24 << 20, transcendentals=0),
    )(
        mix_input,
        mix_gain.reshape(1, width),
        pool_weight,
        pool_scale.reshape(1, width),
        moe_input,
        moe_gain.reshape(1, width),
        expert_ids.T,
        route_score.T,
        expert_gate,
        expert_up,
        expert_down,
        shared_gate,
        shared_up,
        shared_down,
    )


def mixer(mix_input, mix_gain, pool_weight, pool_scale):
    normed = rms_norm(mix_input, mix_gain)
    row_count, width_all = normed.shape
    reach_rows = max(WINDOWS) - 1
    before = passed_along(normed[row_count - reach_rows :], ("ep", "tp"), 1)
    offset = lax.axis_index(("ep", "tp")) * row_count
    pooled = window_means(normed, before, offset)
    difference = (pooled - normed.astype(jnp.float32).reshape(row_count, len(WINDOWS), -1)).astype(
        jnp.bfloat16
    )
    mixed_out = jnp.einsum(
        "sgc,gcd->sgd", difference, pool_weight, preferred_element_type=jnp.float32
    )
    return (mixed_out.reshape(row_count, width_all) * pool_scale).astype(jnp.bfloat16)


def per_device(
    mix_input,
    mix_gain,
    pool_weight,
    pool_scale,
    moe_input,
    moe_gain,
    expert_ids,
    route_score,
    expert_gate,
    expert_up,
    expert_down,
    shared_gate,
    shared_up,
    shared_down,
):
    ep_count, tp_count = lax.axis_size("ep"), lax.axis_size("tp")
    few_experts = (
        ep_count * expert_gate.shape[0] <= 8 * expert_ids.shape[1]
        and ep_count % 2 == 0
        and 2 < ep_count <= 8
        and tp_count == 4
        and expert_gate.shape[0] <= 4
        and expert_ids.shape[1] <= 4
    )
    if few_experts:
        return both_in_one_kernel(
            mix_input,
            mix_gain,
            pool_weight,
            pool_scale,
            moe_input,
            moe_gain,
            expert_ids,
            route_score,
            expert_gate,
            expert_up,
            expert_down,
            shared_gate,
            shared_up,
            shared_down,
        )
    mix_output = mixer(mix_input, mix_gain, pool_weight, pool_scale)
    h_moe = rms_norm(moe_input, moe_gain)
    route_w = route_score / jnp.sum(route_score, axis=1, keepdims=True) * ROUTED_SCALE
    moe_output = routed_by_slots(
        h_moe,
        expert_ids,
        route_w,
        expert_gate,
        expert_up,
        expert_down,
        shared_gate,
        shared_up,
        shared_down,
    )
    return (mix_output, moe_output)


def solution(mesh):
    return jax.shard_map(
        per_device,
        mesh=mesh,
        in_specs=(
            P(("ep", "tp"), None),
            P(),
            P(),
            P(),
            P(("ep", "tp"), None),
            P(),
            P("ep", None),
            P(("ep", "tp"), None),
            P("ep", None, "tp"),
            P("ep", None, "tp"),
            P("ep", "tp", None),
            P(None, "tp"),
            P(None, "tp"),
            P("tp", None),
        ),
        out_specs=(P(("ep", "tp"), None), P(("ep", "tp"), None)),
        check_vma=False,
    )
```
